256 devices in a mesh: ep: 16 (over y, x), tp: 16 (over z, core).
Axes of the slice: x: 4, y: 4, z: 8, core: 2. Of those that a mesh axis runs over, the one named last changes fastest.
Arguments:
- query_rows: bfloat16 [16384, 2048], P('ep', 'tp'), may hold values from -6 to 6
- key_rows: bfloat16 [16384, 2048], P('ep', 'tp'), may hold values from -6 to 6
- value_rows: bfloat16 [16384, 4096], P('ep', 'tp'), may hold values from -6 to 6
- gate_rows: bfloat16 [16384, 4096], P('ep', 'tp'), may hold values from -6 to 6
- log_decay: float32 [16, 16384], P('tp', 'ep'), may hold values from -1.5 to 0
- out_weight: bfloat16 [4096, 2048], P('tp'), may hold values from -0.09375 to 0.09375
- channel_input: bfloat16 [12288, 2048], P(('ep', 'tp')), may hold values from -6 to 6
- norm_gain: float32 [2048], replicated, may hold values from 0.1 to 1.9
- routes: int32 [12288, 2], P(('ep', 'tp')), may hold values from 0 to 31, all different within a row; in each aligned block of 48 rows (0 to 47, 48 to 95, ...) at most 5 rows name the same one
- route_weight: float32 [12288, 2], P(('ep', 'tp')), may hold values from 0.2 to 1.5
- expert_gate: bfloat16 [32, 2048, 2048], P('ep', None, 'tp'), may hold values from -0.125 to 0.125
- expert_up: bfloat16 [32, 2048, 2048], P('ep', None, 'tp'), may hold values from -0.125 to 0.125
- expert_down: bfloat16 [32, 2048, 2048], P('ep', 'tp'), may hold values from -0.125 to 0.125
- shared_gate: bfloat16 [2048, 2048], P(None, 'tp'), may hold values from -0.125 to 0.125
- shared_up: bfloat16 [2048, 2048], P(None, 'tp'), may hold values from -0.125 to 0.125
- shared_down: bfloat16 [2048, 2048], P('tp'), may hold values from -0.125 to 0.125
Outputs:
- mixer_out: bfloat16 [16384, 2048], P(('ep', 'tp'))
- channel_out: bfloat16 [12288, 2048], P(('ep', 'tp'))
The draws below stay inside these ranges and needn't reach their ends.
Inputs may be any that keep to these rules, and one draw needn't show every extreme that they name: `routes`: each row names 2 different experts; among the rows of one device no expert is named more than 5 times, a bound that some block reaches.
All inputs are finite; a program needn't handle non-finite values.
Results may differ from the reference program's by a relative error of at most 0.02.
Values may be sent and summed in bfloat16 or wider, within the bound.
No kernel may reach another device: no remote copies, remote signals or barrier semaphores. Data moves between devices by JAX's collectives and lax.ppermute only.
A program may use at most 128 MiB of HBM per device.

```python
import math
import jax
import jax.numpy as jnp
import numpy as np
from jax import lax

D = 2048
RETENTION_HEADS = 16
DK = 128
DV = 256
BLOCK = 128
TOK_A = 1024
FF = 2048
TOPK = 2
T_M = 48
SEQUENCE_LENGTH = 16384
QK_WIDTH = 2048
V_WIDTH = 4096
EXPERTS = 32
TOKENS_M = 12288
CAP = 5
N_EP = 16
N_TP = 16


def draw_log_decay(key, part):
    key_pieces_list = jax.random.split(jax.random.fold_in(key, 11), 7)
    slow_share = 0.5
    slow_heads = jax.random.uniform(key_pieces_list[0], (RETENTION_HEADS,)) < slow_share
    whole_loss = jax.random.uniform(key_pieces_list[1], (RETENTION_HEADS,), minval=0.1, maxval=0.5)
    fast_rate = jax.random.uniform(key_pieces_list[2], (RETENTION_HEADS,), minval=1.0 / 100.0, maxval=1.0 / 30.0)
    decay_rate = jnp.where(slow_heads, whole_loss / SEQUENCE_LENGTH, fast_rate)
    span_count = SEQUENCE_LENGTH // TOK_A
    block_factor = jnp.exp(jax.random.uniform(key_pieces_list[3], (RETENTION_HEADS, span_count), minval=-0.7, maxval=0.7))
    block_factor = jnp.repeat(block_factor, TOK_A, axis=1)
    jitter = jax.random.uniform(key_pieces_list[4], (RETENTION_HEADS, SEQUENCE_LENGTH), minval=0.5, maxval=1.5)
    steady_level = -(decay_rate[:, None] * block_factor * jitter)
    surge_position = jax.random.randint(key_pieces_list[5], (RETENTION_HEADS, 2), 0, SEQUENCE_LENGTH)
    surge_extent = jnp.log(jax.random.uniform(key_pieces_list[6], (RETENTION_HEADS, 2), minval=0.5, maxval=0.8))
    head_number = jnp.broadcast_to(jnp.arange(RETENTION_HEADS)[:, None], (RETENTION_HEADS, 2))
    surge_list = jnp.zeros((RETENTION_HEADS, SEQUENCE_LENGTH), jnp.float32).at[head_number, surge_position].add(surge_extent)
    return (steady_level + surge_list).astype(jnp.float32)


def block_scale(own_key, shape, cuts, least, largest):
    loudness = 1.0
    for dim, shards_of in cuts:
        steps = jax.random.uniform(jax.random.fold_in(jax.random.fold_in(own_key, 6), dim), (shards_of,), jnp.float32, least / len(cuts), largest / len(cuts))
        loudness = loudness * jnp.repeat(jnp.exp(steps), shape[dim] // shards_of).reshape((-1,) + (1,) * (len(shape) - 1 - dim))
    return loudness


def shared_out(rng, own, number, rows, number_of, top, most, slope):
    sequence = jax.random.permutation(rng, number_of)
    crowded, usual = shares(number_of, rows * top, most, slope, True), shares(number_of, rows * top, most, slope, False)
    places = jnp.arange(number_of)

    def named(tallies, rotation):
        used = int((tallies > 0).sum())
        fixed = max(1, used // 4)
        passed = fixed + (places - fixed + rotation * (used - fixed)) % max(1, number_of - fixed)
        return jnp.zeros((number_of,), jnp.int32).at[sequence[jnp.where(places < fixed, places, passed)]].set(jnp.asarray(tallies, jnp.int32))

    tallies = jnp.where(number % 4 == 0, named(crowded, number // 4), named(usual, number - number // 4 - 1))
    mixed = jax.random.permutation(jax.random.fold_in(own, 3), number_of)
    giver, sink = mixed[0:number_of // 2 * 2:2], mixed[1:number_of // 2 * 2:2]
    slack = jnp.minimum(tallies[giver] - 1, most - tallies[sink]) // 2
    slack = jnp.where((giver == sequence[0]) | (sink == sequence[0]) | (tallies[sink] == 0), 0, jnp.maximum(slack, 0))
    passed = jax.random.randint(jax.random.fold_in(own, 4), (number_of // 2,), 0, 1 << 20) % (slack + 1)
    tallies = tallies.at[giver].add(-passed).at[sink].add(passed)
    members = jnp.searchsorted(jnp.cumsum(tallies), jnp.arange(rows * top), side="right").astype(jnp.int32)
    listing = members.reshape(top, rows).T
    listing = listing[jax.random.permutation(jax.random.fold_in(own, 1), rows)]
    rotation = jax.random.randint(jax.random.fold_in(own, 2), (rows, 1), 0, top)
    return jnp.take_along_axis(listing, (jnp.arange(top)[None, :] + rotation) % top, axis=1)


def shares(amount, total, most, slope, full):
    loads = [(1 << 20) // math.isqrt(standing ** slope) + 1 for standing in range(1, amount + 1)]
    largest = most if full else min(most, max(-(-total // amount), total * loads[0] // sum(loads)))
    least = 1 if total - largest >= amount - 1 else 0
    given, spare = [largest] + [least] * (amount - 1), total - largest - least * (amount - 1)
    while spare > 0:
        free = [i for i in range(1, amount) if given[i] < largest] or [i for i in range(1, amount) if given[i] < most]
        whole, left = sum([loads[i] for i in free]), spare
        for i in free:
            addition = min(most - given[i], max(1, left * loads[i] // whole), spare)
            given[i] = given[i] + addition
            spare = spare - addition
    return np.array(given)


def noise(key, shape, scale, most, pieces=(), kind=jnp.bfloat16):
    values = scale * jax.random.normal(key, shape, jnp.float32)
    if pieces:
        values = values * block_scale(key, shape, pieces, -0.22, 0.18)
    return jnp.clip(values, -most, most).astype(kind)


def setup_inputs(seed: int = 0) -> dict:
    arg_keys = jax.random.split(jax.random.key(seed), 17)
    query_rows = noise(arg_keys[0], (SEQUENCE_LENGTH, QK_WIDTH), 1.0, 6.0, ((0, 16), (1, 16)))
    key_rows = noise(arg_keys[1], (SEQUENCE_LENGTH, QK_WIDTH), 1.0, 6.0, ((0, 16), (1, 16)))
    value_rows = noise(arg_keys[2], (SEQUENCE_LENGTH, V_WIDTH), 1.0, 6.0, ((0, 16), (1, 16)))
    gate_rows = noise(arg_keys[3], (SEQUENCE_LENGTH, V_WIDTH), 1.0, 6.0, ((0, 16), (1, 16)))
    log_decay = draw_log_decay(jax.random.fold_in(arg_keys[16], 71), 0)
    out_weight = noise(arg_keys[5], (V_WIDTH, D), V_WIDTH ** -0.5, 0.09375, ((0, 16),))
    channel_input = noise(arg_keys[6], (TOKENS_M, D), 1.0, 6.0, ((0, 256),))
    norm_gain = jnp.clip(1.0 + 0.18 * jax.random.normal(arg_keys[7], (D,), jnp.float32), 0.1, 1.9)
    routes_keys = jax.random.split(jax.random.fold_in(arg_keys[8], 1), TOKENS_M // T_M)
    routes_turns = jax.random.permutation(jax.random.fold_in(arg_keys[8], 3), TOKENS_M // T_M)
    routes = jax.vmap(lambda own, number: shared_out(jax.random.fold_in(arg_keys[8], 2), own, number, T_M, EXPERTS, TOPK, CAP, 1))(routes_keys, routes_turns).reshape((TOKENS_M, TOPK))
    route_weight = jnp.clip(0.2 + 1.3 * jax.random.uniform(arg_keys[9], (TOKENS_M, TOPK), jnp.float32) ** block_scale(arg_keys[9], (TOKENS_M, TOPK), ((0, 256),), -0.2, 0.2), 0.2, 1.5)
    expert_gate = noise(arg_keys[10], (EXPERTS, D, FF), D ** -0.5, 0.125, ((0, 16), (2, 16)))
    expert_up = noise(arg_keys[11], (EXPERTS, D, FF), D ** -0.5, 0.125, ((0, 16), (2, 16)))
    expert_down = noise(arg_keys[12], (EXPERTS, FF, D), FF ** -0.5, 0.125, ((0, 16), (1, 16)))
    shared_gate = noise(arg_keys[13], (D, FF), D ** -0.5, 0.125, ((1, 16),))
    shared_up = noise(arg_keys[14], (D, FF), D ** -0.5, 0.125, ((1, 16),))
    shared_down = noise(arg_keys[15], (FF, D), FF ** -0.5, 0.125, ((0, 16),))
    return {"query_rows": query_rows, "key_rows": key_rows, "value_rows": value_rows, "gate_rows": gate_rows, "log_decay": log_decay, "out_weight": out_weight, "channel_input": channel_input, "norm_gain": norm_gain, "routes": routes, "route_weight": route_weight, "expert_gate": expert_gate, "expert_up": expert_up, "expert_down": expert_down, "shared_gate": shared_gate, "shared_up": shared_up, "shared_down": shared_down}


epsilon = 1e-06
turn_base = 10000.0

def turn_heads(rows, position):
    half_width = rows.shape[-1] // 2
    inverse = turn_base ** (-jnp.arange(half_width, dtype=jnp.float32) / half_width)
    angles = position[:, None] * inverse[None, :]
    cosine = jnp.cos(angles)[:, None, :]
    sine = jnp.sin(angles)[:, None, :]
    widened = rows.astype(jnp.float32)
    first_half = widened[..., :half_width]
    second_half = widened[..., half_width:]
    turned = jnp.concatenate([first_half * cosine - second_half * sine, second_half * cosine + first_half * sine], axis=-1)
    return turned.astype(jnp.bfloat16)

def blocked_product(left, right, parts):
    width = right.shape[0] // parts

    def add_block(index, total):
        columns = lax.dynamic_slice_in_dim(left, index * width, width, 1)
        block_rows = lax.dynamic_slice_in_dim(right, index * width, width, 0)
        partial_sum = jnp.dot(columns, block_rows, preferred_element_type=jnp.float32).astype(jnp.bfloat16)
        partial_sum = lax.optimization_barrier(partial_sum)
        return total + partial_sum.astype(jnp.float32)
    return lax.fori_loop(0, parts, add_block, jnp.zeros((left.shape[0], right.shape[1]), jnp.float32))

def swiglu_hidden(rows, gate_weight, up_weight):
    gate_part = jnp.dot(rows, gate_weight, preferred_element_type=jnp.float32)
    up_part = jnp.dot(rows, up_weight, preferred_element_type=jnp.float32)
    return (jax.nn.silu(gate_part) * up_part).astype(jnp.bfloat16)

def retention(queries, keys_turned, values, log_decay):
    block_count = SEQUENCE_LENGTH // BLOCK
    query_blocks = queries.reshape(block_count, BLOCK, RETENTION_HEADS, DK)
    key_blocks = keys_turned.reshape(block_count, BLOCK, RETENTION_HEADS, DK)
    value_blocks = values.reshape(block_count, BLOCK, RETENTION_HEADS, DV)
    decay_blocks = jnp.transpose(log_decay.reshape(RETENTION_HEADS, block_count, BLOCK), (1, 0, 2))
    lower = jnp.arange(BLOCK)[:, None] >= jnp.arange(BLOCK)[None, :]
    highest = lax.Precision.HIGHEST

    def advance(state, inputs):
        query_block, key_block, value_block, decay_block = inputs
        running = jnp.cumsum(decay_block, axis=1)
        query_wide = query_block.astype(jnp.float32)
        key_wide = key_block.astype(jnp.float32)
        value_wide = value_block.astype(jnp.float32)
        scores = jnp.einsum('ihk,jhk->hij', query_wide, key_wide, precision=highest)
        spread = running[:, :, None] - running[:, None, :]
        weights = jnp.where(lower, scores * jnp.exp(jnp.where(lower, spread, 0.0)), 0.0).astype(jnp.bfloat16)
        intra = jnp.einsum('hij,jhe->ihe', weights.astype(jnp.float32), value_wide, precision=highest)
        query_decayed = query_wide * jnp.exp(running).T[:, :, None]
        inter = jnp.einsum('ihk,hke->ihe', query_decayed, state, precision=highest)
        block_end = running[:, -1]
        key_decayed = key_wide * jnp.exp(block_end[:, None] - running).T[:, :, None]
        update = jnp.einsum('jhk,jhe->hke', key_decayed, value_wide, precision=highest)
        new_state = jnp.exp(block_end)[:, None, None] * state + update
        return (new_state, intra + inter)
    start_state = jnp.zeros((RETENTION_HEADS, DK, DV), jnp.float32)
    _, outputs = lax.scan(advance, start_state, (query_blocks, key_blocks, value_blocks, decay_blocks))
    return outputs.reshape(SEQUENCE_LENGTH, RETENTION_HEADS, DV)

def reference(query_rows, key_rows, value_rows, gate_rows, log_decay, out_weight, channel_input, norm_gain, routes, route_weight, expert_gate, expert_up, expert_down, shared_gate, shared_up, shared_down):
    position = jnp.arange(SEQUENCE_LENGTH, dtype=jnp.int32).astype(jnp.float32)
    queries = turn_heads(query_rows.reshape(SEQUENCE_LENGTH, RETENTION_HEADS, DK), position)
    keys_turned = turn_heads(key_rows.reshape(SEQUENCE_LENGTH, RETENTION_HEADS, DK), position)
    retained = retention(queries, keys_turned, value_rows.reshape(SEQUENCE_LENGTH, RETENTION_HEADS, DV), log_decay)
    scaled = retained * lax.rsqrt(lax.optimization_barrier(jnp.mean(retained * retained, axis=-1, keepdims=True)) + epsilon)
    gate_wide = gate_rows.astype(jnp.float32).reshape(SEQUENCE_LENGTH, RETENTION_HEADS, DV)
    gated = (jax.nn.silu(gate_wide) * scaled).astype(jnp.bfloat16).reshape(SEQUENCE_LENGTH, RETENTION_HEADS * DV)
    mixer_out = blocked_product(gated, out_weight, N_TP).astype(jnp.bfloat16)
    widened = channel_input.astype(jnp.float32)
    normed = (widened * lax.rsqrt(lax.optimization_barrier(jnp.mean(widened * widened, axis=-1, keepdims=True)) + epsilon) * norm_gain).astype(jnp.bfloat16)
    shared_result = blocked_product(swiglu_hidden(normed, shared_gate, shared_up), shared_down, N_TP)
    flat_expert = routes.reshape(-1)
    assign_count = flat_expert.shape[0]
    flat_token = jnp.arange(assign_count, dtype=jnp.int32) // TOPK
    flat_weight = route_weight.reshape(-1)
    limit = N_EP * N_TP * CAP

    def add_expert(total, expert):
        chosen = jnp.nonzero(flat_expert == expert, size=limit, fill_value=assign_count)[0].astype(jnp.int32)
        valid = chosen < assign_count
        safe = jnp.minimum(chosen, assign_count - 1)
        token_index = flat_token[safe]
        weight = jnp.where(valid, flat_weight[safe], 0.0)
        hidden = swiglu_hidden(normed[token_index], expert_gate[expert], expert_up[expert])
        result = blocked_product(hidden, expert_down[expert], N_TP).astype(jnp.bfloat16)
        result = lax.optimization_barrier(result)
        return (total.at[token_index].add(weight[:, None] * result.astype(jnp.float32)), None)
    routed, _ = lax.scan(add_expert, jnp.zeros((TOKENS_M, D), jnp.float32), jnp.arange(EXPERTS, dtype=jnp.int32))
    channel_out = (shared_result + routed).astype(jnp.bfloat16)
    return (mixer_out, channel_out)
```

```python
import jax
import jax.numpy as jnp
from jax import lax
from jax.experimental import pallas as pl
from jax.experimental.pallas import tpu as pltpu
from jax.sharding import Mesh
from jax.sharding import PartitionSpec as P

BLOCK = 128
EP = ("ep_0", "ep_1")
EP_TP = ("ep_0", "ep_1", "tp")
LANES = 128
SLOTS = 8

epsilon = 1e-06
turn_base = 10000.0
bf16 = jnp.bfloat16
f32 = jnp.float32


def carried_in(log_total, state, axes):
    before_log, before = jnp.zeros_like(log_total), jnp.zeros_like(state)
    for axis in reversed(axes):
        length, index = lax.axis_size(axis), lax.axis_index(axis)
        high = log_total.astype(bf16)
        low = (log_total - high.astype(f32)).astype(bf16)
        width = state.shape[1]
        marks = jnp.arange(16)[:, None]
        extra = jnp.where(marks == 0, high, jnp.where(marks == 1, low, jnp.zeros((), bf16)))
        packed = jnp.concatenate([state.astype(bf16), jnp.broadcast_to(extra, (16, width))], axis=0)
        pieces = lax.all_gather(packed, axis)
        rows = state.shape[0]
        inside_log, inside = jnp.zeros_like(log_total), jnp.zeros_like(state)
        total_log, total = inside_log, inside
        for k in range(length):
            passed = k < index
            piece_log = pieces[k, rows, 0].astype(f32) + pieces[k, rows + 1, 0].astype(f32)
            total = jnp.exp(piece_log) * total + pieces[k, :rows].astype(f32)
            total_log = total_log + piece_log
            inside = jnp.where(passed, total, inside)
            inside_log = jnp.where(passed, total_log, inside_log)
        before = jnp.exp(before_log) * inside + before
        before_log = before_log + inside_log
        log_total, state = total_log, total
    return before


def turn_tables(position, half_width):
    inverse = turn_base ** (-jnp.arange(half_width, dtype=f32) / half_width)
    angles = position[:, None] * inverse[None, :]
    return jnp.cos(angles), jnp.sin(angles)


def turn_head(rows, cosine, sine):
    half_width = rows.shape[-1] // 2
    widened = rows.astype(f32)
    first_half, second_half = widened[:, :half_width], widened[:, half_width:]
    turned = jnp.concatenate(
        [first_half * cosine - second_half * sine, second_half * cosine + first_half * sine],
        axis=-1,
    )
    return turned.astype(bf16)


def silu(v):
    return v / (1.0 + jnp.exp(-v))


def mixer_kernel(gated_ref, weight_ref, out_ref):
    groups, rows, width = gated_ref.shape
    left = gated_ref[...].reshape(groups * rows, width)
    product = jnp.dot(left, weight_ref[...], preferred_element_type=f32)
    out_ref[...] = product.astype(bf16).reshape(out_ref.shape)


def expert_kernel(x_ref, first_ref, down_ref, held_ref, out_ref):
    del held_ref
    groups, rows, width = x_ref.shape
    model_width = out_ref.shape[-1]
    x = x_ref[...].reshape(groups * rows, width)
    hidden = jnp.dot(x[:, :model_width], first_ref[0], preferred_element_type=f32)
    part = hidden.shape[1] // 4
    extra = x[:, model_width:].astype(f32)
    weight = extra[:, 0:1] + extra[:, 1:2]
    own = extra[:, 2:3]
    routed = silu(hidden[:, :part]) * hidden[:, part : 2 * part] * weight
    shared = silu(hidden[:, 2 * part : 3 * part]) * hidden[:, 3 * part :] * own
    both = jnp.concatenate([routed, shared], axis=1).astype(bf16)
    product = jnp.dot(both, down_ref[0], preferred_element_type=f32)
    out_ref[...] = product.astype(bf16).reshape(out_ref.shape)


def retention(query_rows, key_rows, value_rows, gate_rows, log_decay):
    tokens = query_rows.shape[0]
    count = tokens // BLOCK
    start = lax.axis_index(EP) * tokens
    position = (start + jnp.arange(tokens, dtype=jnp.int32)).astype(f32)
    cosine, sine = turn_tables(position, query_rows.shape[1] // 2)
    queries = turn_head(query_rows, cosine, sine).reshape(count, BLOCK, -1)
    keys_turned = turn_head(key_rows, cosine, sine).reshape(count, BLOCK, -1)
    values = value_rows.reshape(count, BLOCK, -1)
    decay = log_decay.reshape(count, BLOCK)
    lower = jnp.arange(BLOCK)[:, None] >= jnp.arange(BLOCK)[None, :]
    running = jnp.dot(decay, lower.T.astype(f32), precision=lax.Precision.HIGHEST)
    block_end = running[:, -1]
    tail = jnp.exp(block_end[:, None] - running)
    updates = jnp.einsum(
        "njk,nje->nke",
        (keys_turned.astype(f32) * tail[..., None]).astype(bf16),
        values,
        preferred_element_type=f32,
    )
    state = jnp.zeros(updates.shape[1:], f32)
    before = []
    for n in range(count):
        before.append(state)
        state = jnp.exp(block_end[n]) * state + updates[n]
    entry = carried_in(jnp.sum(block_end), state, EP)
    offsets = jnp.cumsum(block_end) - block_end
    state_before = jnp.stack(before) + jnp.exp(offsets)[:, None, None] * entry[None]
    scores = jnp.einsum("nik,njk->nij", queries, keys_turned, preferred_element_type=f32)
    spread = running[:, :, None] - running[:, None, :]
    weights = jnp.where(lower, scores * jnp.exp(jnp.where(lower, spread, 0.0)), 0.0).astype(bf16)
    retained = jnp.einsum("nij,nje->nie", weights, values, preferred_element_type=f32)
    retained = retained + jnp.einsum(
        "nik,nke->nie",
        (queries.astype(f32) * jnp.exp(running)[..., None]).astype(bf16),
        state_before.astype(bf16),
        preferred_element_type=f32,
    )
    retained = retained.reshape(tokens, -1)
    scaled = retained * lax.rsqrt(jnp.mean(retained * retained, axis=-1, keepdims=True) + epsilon)
    return (jax.nn.silu(gate_rows.astype(f32)) * scaled).astype(bf16)


def local(
    query_rows,
    key_rows,
    value_rows,
    gate_rows,
    log_decay,
    out_weight,
    channel_input,
    norm_gain,
    routes,
    route_weight,
    expert_gate,
    expert_up,
    expert_down,
    shared_gate,
    shared_up,
    shared_down,
):
    tokens_dev = query_rows.shape[0]
    tokens_here, topk = routes.shape
    model_width = channel_input.shape[1]
    local_experts, _, hidden_part = expert_gate.shape
    ep_count = lax.axis_size(EP)
    tp_count = lax.axis_size("tp")
    experts_all = ep_count * local_experts
    picks = tokens_here * topk
    capacity = picks // experts_all + max(2, picks // (3 * experts_all))
    slot_count = experts_all * SLOTS

    widened = channel_input.astype(f32)
    normed = (
        widened * lax.rsqrt(jnp.mean(widened * widened, axis=-1, keepdims=True) + epsilon) * norm_gain
    ).astype(bf16)
    flat = routes.reshape(-1)
    order = jnp.arange(picks, dtype=jnp.int32)
    same = (flat[:, None] == flat[None, :]) & (order[None, :] < order[:, None])
    slots = flat * SLOTS + jnp.sum(same.astype(jnp.int32), axis=1)
    placing = (jnp.arange(slot_count, dtype=jnp.int32)[:, None] == slots[None, :]).astype(bf16)
    placing_rows = placing.reshape(slot_count, tokens_here, topk).sum(axis=2)
    flat_weight = route_weight.reshape(-1)
    high = flat_weight.astype(bf16)
    low = (flat_weight - high.astype(f32)).astype(bf16)
    mark = (order % topk == 0).astype(bf16)
    lane = jnp.arange(LANES)[None, :]
    extra = jnp.where(
        lane == 0,
        high[:, None],
        jnp.where(lane == 1, low[:, None], jnp.where(lane == 2, mark[:, None], jnp.zeros((), bf16))),
    )
    outgoing = jnp.concatenate(
        [
            jnp.dot(placing_rows, normed, preferred_element_type=f32).astype(bf16),
            jnp.dot(placing, extra, preferred_element_type=f32).astype(bf16),
        ],
        axis=1,
    )
    width = model_width + LANES
    outgoing = outgoing.reshape(ep_count, local_experts * SLOTS, width)
    arrived = lax.all_to_all(outgoing, EP, split_axis=0, concat_axis=0, tiled=True)
    arrived = arrived.reshape(ep_count, local_experts, SLOTS, width)[:, :, :capacity]
    arrived = jnp.transpose(arrived, (1, 2, 0, 3)).reshape(1, -1, width)
    gathered = lax.all_gather(arrived, "tp", axis=0, tiled=True)
    routed_rows = gathered.shape[1]

    gated = retention(query_rows, key_rows, value_rows, gate_rows, log_decay)
    mixer_rows = tokens_dev // tp_count
    total_rows = routed_rows + mixer_rows
    step = 32
    buffer = pl.pallas_call(
        mixer_kernel,
        grid=(mixer_rows // step,),
        in_specs=[
            pl.BlockSpec((tp_count, step, gated.shape[1]), lambda i: (0, i, 0)),
            pl.BlockSpec(out_weight.shape, lambda i: (0, 0)),
        ],
        out_specs=pl.BlockSpec(
            (tp_count, step, model_width), lambda i: (0, routed_rows // step + i, 0)
        ),
        out_shape=jax.ShapeDtypeStruct((tp_count, total_rows, model_width), bf16),
    )(gated.reshape(tp_count, mixer_rows, -1), out_weight)

    spread = (local_experts,) + shared_gate.shape
    first = jnp.concatenate(
        [
            expert_gate,
            expert_up,
            jnp.broadcast_to(shared_gate, spread),
            jnp.broadcast_to(shared_up, spread),
        ],
        axis=2,
    )
    down = jnp.concatenate(
        [expert_down, jnp.broadcast_to(shared_down, (local_experts,) + shared_down.shape)], axis=1
    )
    each = routed_rows // local_experts
    groups = 4
    buffer = pl.pallas_call(
        expert_kernel,
        grid=(local_experts, tp_count // groups),
        in_specs=[
            pl.BlockSpec((groups, each, width), lambda e, t: (t, e, 0)),
            pl.BlockSpec((1,) + first.shape[1:], lambda e, t: (e, 0, 0)),
            pl.BlockSpec((1,) + down.shape[1:], lambda e, t: (e, 0, 0)),
            pl.BlockSpec(memory_space=pl.ANY),
        ],
        out_specs=pl.BlockSpec((groups, each, model_width), lambda e, t: (t, e, 0)),
        out_shape=jax.ShapeDtypeStruct(buffer.shape, bf16),
        input_output_aliases={3: 0},
        compiler_params=pltpu.CompilerParams(vmem_limit_bytes=50 * 2**20),
    )(gathered, first, down, buffer)

    summed = lax.psum_scatter(buffer, "tp", scatter_dimension=0, tiled=True)[0]
    mixer_out = summed[routed_rows:]
    back = summed[:routed_rows].reshape(local_experts, capacity, ep_count, model_width)
    back = jnp.transpose(back, (2, 0, 1, 3))
    back = jnp.pad(back, ((0, 0), (0, 0), (0, SLOTS - capacity), (0, 0)))
    back = back.reshape(ep_count, local_experts * SLOTS, model_width)
    returned = lax.all_to_all(back, EP, split_axis=0, concat_axis=0, tiled=True)
    returned = returned.reshape(slot_count, model_width)
    channel = jnp.dot(placing_rows.T, returned, preferred_element_type=f32)
    return (mixer_out, channel.astype(bf16))


def solution(mesh):
    split = Mesh(mesh.devices.reshape(4, 4, mesh.shape["tp"]), ("ep_0", "ep_1", "tp"))
    return jax.shard_map(
        local,
        mesh=split,
        in_specs=(
            P(EP, "tp"),
            P(EP, "tp"),
            P(EP, "tp"),
            P(EP, "tp"),
            P("tp", EP),
            P("tp", None),
            P(EP_TP, None),
            P(),
            P(EP_TP, None),
            P(EP_TP, None),
            P(EP, None, "tp"),
            P(EP, None, "tp"),
            P(EP, "tp", None),
            P(None, "tp"),
            P(None, "tp"),
            P("tp", None),
        ),
        out_specs=(P(EP_TP, None), P(EP_TP, None)),
        check_vma=False,
    )
```

```python
import jax
import jax.numpy as jnp
from jax import lax
from jax.experimental import pallas as pl
from jax.experimental.pallas import tpu as pltpu
from jax.sharding import Mesh
from jax.sharding import PartitionSpec as P

BLOCK = 128
EP = ("ep_0", "ep_1")
TP = ("z", "core")
EP_TP = EP + TP
LANES = 128
SLOTS = 8
STRIP = 32

epsilon = 1e-06
turn_base = 10000.0
bf16 = jnp.bfloat16
f32 = jnp.float32


def silu(v):
    return v / (1.0 + jnp.exp(-v))


def expert_kernel(x_ref, first_ref, down_ref, held_ref, out_ref):
    del held_ref
    groups, rows, width = x_ref.shape
    model_width = out_ref.shape[-1]
    x = x_ref[...].reshape(groups * rows, width)
    hidden = jnp.dot(x[:, :model_width], first_ref[0], preferred_element_type=f32)
    part = hidden.shape[1] // 4
    extra = x[:, model_width:].astype(f32)
    weight = extra[:, 0:1] + extra[:, 1:2]
    own = extra[:, 2:3]
    routed = silu(hidden[:, :part]) * hidden[:, part : 2 * part] * weight
    shared = silu(hidden[:, 2 * part : 3 * part]) * hidden[:, 3 * part :] * own
    both = jnp.concatenate([routed, shared], axis=1).astype(bf16)
    product = jnp.dot(both, down_ref[0], preferred_element_type=f32)
    out_ref[...] = product.astype(bf16).reshape(out_ref.shape)


def masks():
    row = lax.broadcasted_iota(jnp.int32, (BLOCK, BLOCK), 0)
    column = lax.broadcasted_iota(jnp.int32, (BLOCK, BLOCK), 1)
    return row == column, row >= column


def upright(line, same):
    return jnp.sum(jnp.where(same, line, 0.0), axis=1, keepdims=True)


def advance(state, keys, values, line, column):
    end = line[:, BLOCK - 1 :]
    decayed = (keys.astype(f32) * jnp.exp(end - column)).astype(bf16)
    update = lax.dot_general(
        decayed, values, (((0,), (0,)), ((), ())), preferred_element_type=f32
    )
    return jnp.exp(end) * state + update


def state_kernel(q_ref, k_ref, v_ref, cos_ref, sin_ref, line_ref, qt_ref, kt_ref, out_ref, state_ref, log_ref):
    @pl.when(pl.program_id(0) == 0)
    def _():
        state_ref[...] = jnp.zeros_like(state_ref)
        log_ref[...] = jnp.zeros_like(log_ref)

    cosine, sine = cos_ref[...], sin_ref[...]
    half = q_ref.shape[1] // 2
    q, k = q_ref[...].astype(f32), k_ref[...].astype(f32)
    qt_ref[...] = (q * cosine + pltpu.roll(q, half, 1) * sine).astype(bf16)
    keys = (k * cosine + pltpu.roll(k, half, 1) * sine).astype(bf16)
    kt_ref[...] = keys
    line = line_ref[0]
    same, _ = masks()
    state_ref[...] = advance(state_ref[...], keys, v_ref[...], line, upright(line, same))
    log_ref[...] = log_ref[...] + line[:, BLOCK - 1 :]

    @pl.when(pl.program_id(0) == pl.num_programs(0) - 1)
    def _():
        rows = state_ref.shape[0]
        total = log_ref[...]
        high = total.astype(bf16).astype(f32)
        mark = lax.broadcasted_iota(jnp.int32, total.shape, 0)
        extra = jnp.where(mark == 0, high, jnp.where(mark == 1, total - high, 0.0))
        out_ref[:rows] = state_ref[...].astype(bf16)
        out_ref[rows:] = extra.astype(bf16)


def mixer_kernel(
    place_ref, pieces_ref, q_ref, k_ref, v_ref, gate_ref, line_ref, weight_ref, out_ref, state_ref, mixed_ref
):
    rows = state_ref.shape[0]
    strip = pl.program_id(1)

    @pl.when((pl.program_id(0) == 0) & (strip == 0))
    def _():
        state_ref[...] = jnp.zeros_like(state_ref)

        def enter(k, _):
            log = pieces_ref[k, rows : rows + 16, :].astype(f32)
            decay = jnp.exp(log[0:1, :] + log[1:2, :])
            state_ref[...] = decay * state_ref[...] + pieces_ref[k, :rows, :].astype(f32)
            return 0

        lax.fori_loop(0, place_ref[0], enter, 0)

    @pl.when(strip == 0)
    def _():
        queries, keys, values = q_ref[...], k_ref[...], v_ref[...]
        line = line_ref[0]
        same, lower = masks()
        column = upright(line, same)
        scores = lax.dot_general(
            queries, keys, (((1,), (1,)), ((), ())), preferred_element_type=f32
        )
        spread = jnp.where(lower, column - line, 0.0)
        weights = jnp.where(lower, scores * jnp.exp(spread), 0.0).astype(bf16)
        state = state_ref[...]
        retained = jnp.dot(weights, values, preferred_element_type=f32)
        retained = retained + jnp.dot(
            (queries.astype(f32) * jnp.exp(column)).astype(bf16),
            state.astype(bf16),
            preferred_element_type=f32,
        )
        state_ref[...] = advance(state, keys, values, line, column)
        mean = jnp.mean(retained * retained, axis=1, keepdims=True)
        gated = (silu(gate_ref[...].astype(f32)) * (retained * lax.rsqrt(mean + epsilon))).astype(bf16)
        mixed = jnp.dot(gated, weight_ref[...], preferred_element_type=f32)
        mixed_ref[...] = mixed.astype(bf16)

    for k in range(BLOCK // 2 // STRIP):

        @pl.when(strip == k)
        def _():
            for half in range(2):
                first = half * (BLOCK // 2) + k * STRIP
                out_ref[half] = mixed_ref[first : first + STRIP]


def retention(query_rows, key_rows, value_rows, gate_rows, log_decay, out_weight, rows_before):
    tokens, key_width = query_rows.shape
    value_width = value_rows.shape[1]
    model_width = out_weight.shape[1]
    count = tokens // BLOCK
    ep_count = lax.axis_size(EP)
    members = lax.axis_size(TP)
    start = lax.axis_index(EP) * tokens
    position = (start + jnp.arange(tokens, dtype=jnp.int32)).astype(f32)
    half_width = key_width // 2
    entry = jnp.arange(key_width)
    inverse = turn_base ** (-(entry % half_width).astype(f32) / half_width)
    angles = position[:, None] * inverse[None, :]
    cosine = jnp.cos(angles)
    sine = jnp.where(entry < half_width, -1.0, 1.0) * jnp.sin(angles)
    order = jnp.arange(BLOCK)
    upper = (order[:, None] <= order[None, :]).astype(f32)
    running = jnp.dot(log_decay.reshape(count, BLOCK), upper, precision=lax.Precision.HIGHEST)
    running = running.reshape(count, 1, BLOCK)

    def rows_of(width):
        return pl.BlockSpec((BLOCK, width), lambda n, *_: (n, 0))

    line = pl.BlockSpec((1, 1, BLOCK), lambda n, *_: (n, 0, 0))
    queries, keys, piece = pl.pallas_call(
        state_kernel,
        grid=(count,),
        in_specs=[rows_of(key_width)] * 2 + [rows_of(value_width)] + [rows_of(key_width)] * 2 + [line],
        out_specs=[
            rows_of(key_width),
            rows_of(key_width),
            pl.BlockSpec((key_width + 16, value_width), lambda n: (0, 0)),
        ],
        out_shape=[
            jax.ShapeDtypeStruct((tokens, key_width), bf16),
            jax.ShapeDtypeStruct((tokens, key_width), bf16),
            jax.ShapeDtypeStruct((key_width + 16, value_width), bf16),
        ],
        scratch_shapes=[
            pltpu.VMEM((key_width, value_width), f32),
            pltpu.VMEM((16, value_width), f32),
        ],
    )(query_rows, key_rows, value_rows, cosine, sine, running)
    pieces = lax.all_to_all(
        jnp.broadcast_to(piece, (ep_count,) + piece.shape), EP, split_axis=0, concat_axis=0, tiled=True
    )
    where = jnp.reshape(lax.axis_index(EP), (1,)).astype(jnp.int32)
    strips = BLOCK // 2 // STRIP
    return pl.pallas_call(
        mixer_kernel,
        grid_spec=pltpu.PrefetchScalarGridSpec(
            num_scalar_prefetch=1,
            grid=(count, strips),
            in_specs=[
                pl.BlockSpec(pieces.shape, lambda n, *_: (0, 0, 0)),
                rows_of(key_width),
                rows_of(key_width),
                rows_of(value_width),
                rows_of(value_width),
                line,
                pl.BlockSpec(out_weight.shape, lambda n, *_: (0, 0)),
            ],
            out_specs=pl.BlockSpec(
                (2, STRIP, model_width), lambda n, k, *_: (n, rows_before // STRIP + k, 0)
            ),
            scratch_shapes=[
                pltpu.VMEM((key_width, value_width), f32),
                pltpu.VMEM((BLOCK, model_width), bf16),
            ],
        ),
        out_shape=jax.ShapeDtypeStruct((members, rows_before + tokens // members, model_width), bf16),
        compiler_params=pltpu.CompilerParams(vmem_limit_bytes=40 * 2**20),
    )(where, pieces, queries, keys, value_rows, gate_rows, running, out_weight)


def local(
    query_rows,
    key_rows,
    value_rows,
    gate_rows,
    log_decay,
    out_weight,
    channel_input,
    norm_gain,
    routes,
    route_weight,
    expert_gate,
    expert_up,
    expert_down,
    shared_gate,
    shared_up,
    shared_down,
):
    tokens_dev = query_rows.shape[0]
    tokens_here, topk = routes.shape
    model_width = channel_input.shape[1]
    local_experts, _, hidden_part = expert_gate.shape
    ep_count = lax.axis_size(EP)
    experts_all = ep_count * local_experts
    picks = tokens_here * topk
    capacity = picks // experts_all + max(2, picks // (3 * experts_all))
    slot_count = experts_all * SLOTS

    widened = channel_input.astype(f32)
    normed = (
        widened * lax.rsqrt(jnp.mean(widened * widened, axis=-1, keepdims=True) + epsilon) * norm_gain
    ).astype(bf16)
    flat = routes.reshape(-1)
    order = jnp.arange(picks, dtype=jnp.int32)
    same = (flat[:, None] == flat[None, :]) & (order[None, :] < order[:, None])
    rank = jnp.sum(same.astype(jnp.int32), axis=1)
    slots = ((flat % local_experts) * ep_count + flat // local_experts) * SLOTS + rank
    placing = (jnp.arange(slot_count, dtype=jnp.int32)[:, None] == slots[None, :]).astype(bf16)
    placing_rows = placing.reshape(slot_count, tokens_here, topk).sum(axis=2)
    flat_weight = route_weight.reshape(-1)
    high = flat_weight.astype(bf16)
    low = (flat_weight - high.astype(f32)).astype(bf16)
    mark = (order % topk == 0).astype(bf16)
    lane = jnp.arange(LANES)[None, :]
    extra = jnp.where(
        lane == 0,
        high[:, None],
        jnp.where(lane == 1, low[:, None], jnp.where(lane == 2, mark[:, None], jnp.zeros((), bf16))),
    )
    outgoing = jnp.concatenate(
        [
            jnp.dot(placing_rows, normed, preferred_element_type=f32).astype(bf16),
            jnp.dot(placing, extra, preferred_element_type=f32).astype(bf16),
        ],
        axis=1,
    )
    width = model_width + LANES
    outgoing = outgoing.reshape(local_experts, ep_count, SLOTS, width)
    gathered = []
    for e in range(local_experts):
        arrived = lax.all_to_all(outgoing[e], EP, split_axis=0, concat_axis=0, tiled=True)
        arrived = jnp.transpose(arrived[:, :capacity], (1, 0, 2)).reshape(1, -1, width)
        gathered.append(lax.all_gather(arrived, TP, axis=0, tiled=True))
    each = gathered[0].shape[1]
    routed_rows = local_experts * each

    buffer = retention(
        query_rows, key_rows, value_rows, gate_rows, log_decay, out_weight, routed_rows
    )
    spread = (local_experts,) + shared_gate.shape
    first = jnp.concatenate(
        [
            expert_gate,
            expert_up,
            jnp.broadcast_to(shared_gate, spread),
            jnp.broadcast_to(shared_up, spread),
        ],
        axis=2,
    )
    down = jnp.concatenate(
        [expert_down, jnp.broadcast_to(shared_down, (local_experts,) + shared_down.shape)], axis=1
    )
    groups = 4
    for e in range(local_experts):
        buffer = pl.pallas_call(
            expert_kernel,
            grid=(buffer.shape[0] // groups,),
            in_specs=[
                pl.BlockSpec((groups, each, width), lambda t: (t, 0, 0)),
                pl.BlockSpec((1,) + first.shape[1:], lambda t, e=e: (e, 0, 0)),
                pl.BlockSpec((1,) + down.shape[1:], lambda t, e=e: (e, 0, 0)),
                pl.BlockSpec(memory_space=pl.ANY),
            ],
            out_specs=pl.BlockSpec((groups, each, model_width), lambda t, e=e: (t, e, 0)),
            out_shape=jax.ShapeDtypeStruct(buffer.shape, bf16),
            input_output_aliases={3: 0},
            compiler_params=pltpu.CompilerParams(vmem_limit_bytes=50 * 2**20),
        )(gathered[e], first, down, buffer)

    summed = lax.psum_scatter(buffer, TP, scatter_dimension=0, tiled=True)[0]
    mixer_out = summed[routed_rows:]
    back = summed[:routed_rows].reshape(local_experts, capacity, ep_count, model_width)
    back = jnp.transpose(back, (2, 0, 1, 3))
    back = jnp.pad(back, ((0, 0), (0, 0), (0, SLOTS - capacity), (0, 0)))
    back = back.reshape(ep_count, local_experts * SLOTS, model_width)
    returned = lax.all_to_all(back, EP, split_axis=0, concat_axis=0, tiled=True)
    returned = returned.reshape(slot_count, model_width)
    fetch = placing_rows.reshape(local_experts, ep_count, SLOTS, tokens_here)
    fetch = jnp.transpose(fetch, (1, 0, 2, 3)).reshape(slot_count, tokens_here)
    channel = jnp.dot(fetch.T, returned, preferred_element_type=f32)
    return (mixer_out, channel.astype(bf16))


def solution(mesh):
    cores = 2
    split = Mesh(
        mesh.devices.reshape(4, 4, mesh.shape["tp"] // cores, cores), EP_TP
    )
    return jax.shard_map(
        local,
        mesh=split,
        in_specs=(
            P(EP, TP),
            P(EP, TP),
            P(EP, TP),
            P(EP, TP),
            P(TP, EP),
            P(TP, None),
            P(EP_TP, None),
            P(),
            P(EP_TP, None),
            P(EP_TP, None),
            P(EP, None, TP),
            P(EP, None, TP),
            P(EP, TP, None),
            P(None, TP),
            P(None, TP),
            P(TP, None),
        ),
        out_specs=(P(EP_TP, None), P(EP_TP, None)),
        check_vma=False,
    )
```

```python
import functools

import jax
import jax.numpy as jnp
from jax import lax
from jax.experimental import pallas as pl
from jax.experimental.pallas import tpu as pltpu
from jax.sharding import Mesh
from jax.sharding import PartitionSpec as P


BLOCK = 128
EP = ("ep_0", "ep_1")
TP = ("z", "core")
EP_TP = EP + TP
LANES = 128
SLOTS = 8
STRIP = 16

epsilon = 1e-06
turn_base = 10000.0
bf16 = jnp.bfloat16
f32 = jnp.float32


def silu(v):
    return v / (1.0 + jnp.exp(-v))


def hidden_kernel(gate_ref, up_ref, down_ref, x_ref, *refs):
    held, (out_ref, first_ref) = refs[:-2], refs[-2:]
    part = gate_ref.shape[-1]

    @pl.when(pl.program_id(0) == 0)
    def _():
        first_ref[:, :part] = gate_ref[0]
        first_ref[:, part:] = up_ref[0]

    hidden = jnp.dot(x_ref[...], first_ref[...], preferred_element_type=f32)
    act = (silu(hidden[:, :part]) * hidden[:, part:]).astype(bf16)
    total = jnp.dot(act, down_ref[0], preferred_element_type=f32)
    for ref in held:
        total = total + ref[...].astype(f32)
    out_ref[...] = total.astype(bf16)


def gated_mlp(x, gate, up, down, which, held=()):
    rows = x.shape[0]
    model_width, part = gate.shape[1:]
    step = rows // 2
    block = pl.BlockSpec((step, model_width), lambda i: (i, 0))
    wide = pl.BlockSpec((1, model_width, part), lambda i: (which, 0, 0))
    return pl.pallas_call(
        hidden_kernel,
        grid=(rows // step,),
        in_specs=[
            wide,
            wide,
            pl.BlockSpec((1, part, model_width), lambda i: (which, 0, 0)),
            block,
        ]
        + [block] * len(held),
        out_specs=block,
        out_shape=pltpu.HBM((rows, model_width), bf16),
        scratch_shapes=[pltpu.VMEM((model_width, 2 * part), bf16)],
        compiler_params=pltpu.CompilerParams(vmem_limit_bytes=40 * 2**20),
    )(gate, up, down, x, *held)


def column_codes(shape, expert, experts_here, capacity, blocks):
    column = lax.broadcasted_iota(jnp.int32, shape, 1)
    block_rows = blocks * capacity
    target, rest = column // block_rows, column % block_rows
    block, rank = rest // capacity, rest % capacity
    return target * (experts_here * capacity) + expert * capacity + rank, block


def place_kernel(expert, experts_here, capacity, blocks, x_ref, meta_ref, out_ref, hits_ref):
    @pl.when(pl.program_id(0) == 0)
    def _():
        meta = meta_ref[...].astype(f32).astype(jnp.int32)
        shape = hits_ref.shape
        code, block = column_codes(shape, expert, experts_here, capacity, blocks)
        row = lax.broadcasted_iota(jnp.int32, shape, 0) // (shape[0] // blocks)
        hit = ((meta[:, 0:1] == code) | (meta[:, 1:2] == code)) & (row == block)
        hits_ref[...] = jnp.where(hit, 1.0, 0.0).astype(bf16)

    out_ref[...] = lax.dot_general(
        hits_ref[...], x_ref[...], (((0,), (0,)), ((), ())), preferred_element_type=f32
    ).astype(bf16)


def place(rows, expert, experts_here, capacity, blocks, targets):
    count, width = rows.shape
    model_width = width - LANES
    step = 512
    out_rows = targets * blocks * capacity
    return pl.pallas_call(
        functools.partial(place_kernel, expert, experts_here, capacity, blocks),
        grid=(model_width // step,),
        in_specs=[
            pl.BlockSpec((count, step), lambda i: (0, i)),
            pl.BlockSpec((count, LANES), lambda i: (0, model_width // LANES)),
        ],
        out_specs=pl.BlockSpec((out_rows, step), lambda i: (0, i)),
        out_shape=pltpu.HBM((out_rows, model_width), bf16),
        scratch_shapes=[pltpu.VMEM((count, out_rows), bf16)],
        compiler_params=pltpu.CompilerParams(vmem_limit_bytes=40 * 2**20),
    )(rows, rows)


def collect_kernel(expert, experts_here, capacity, blocks, meta_ref, back_ref, *refs):
    held, (out_ref, share_ref) = refs[:-2], refs[-2:]

    @pl.when(pl.program_id(0) == 0)
    def _():
        meta = meta_ref[...].astype(f32)
        slot = meta.astype(jnp.int32)
        shape = share_ref.shape
        code, block = column_codes(shape, expert, experts_here, capacity, blocks)
        here = lax.broadcasted_iota(jnp.int32, shape, 0) // (shape[0] // blocks) == block
        first = jnp.where((slot[:, 0:1] == code) & here, meta[:, 2:3], 0.0)
        second = jnp.where((slot[:, 1:2] == code) & here, meta[:, 3:4], 0.0)
        share_ref[...] = (first + second).astype(bf16)

    total = jnp.dot(share_ref[...], back_ref[...], preferred_element_type=f32)
    for ref in held:
        total = total + ref[...].astype(f32)
    out_ref[...] = total.astype(out_ref.dtype)


def collect(rows, back, held, expert, experts_here, capacity, blocks, kind):
    count, width = rows.shape
    model_width = width - LANES
    step = 512
    return pl.pallas_call(
        functools.partial(collect_kernel, expert, experts_here, capacity, blocks),
        grid=(model_width // step,),
        in_specs=[
            pl.BlockSpec((count, LANES), lambda i: (0, model_width // LANES)),
            pl.BlockSpec((back.shape[0], step), lambda i: (0, i)),
        ]
        + [pl.BlockSpec((count, step), lambda i: (0, i))] * len(held),
        out_specs=pl.BlockSpec((count, step), lambda i: (0, i)),
        out_shape=jax.ShapeDtypeStruct((count, model_width), kind),
        scratch_shapes=[pltpu.VMEM((count, back.shape[0]), bf16)],
        compiler_params=pltpu.CompilerParams(vmem_limit_bytes=40 * 2**20),
    )(rows, back, *held)


def shift(x, axis, by):
    size = lax.axis_size(axis)
    return lax.ppermute(x, axis, [(i, (i + by) % size) for i in range(size)])


def swap(x):
    return lax.ppermute(x, "core", [(0, 1), (1, 0)])


def ring_gather(x, axis):
    size = lax.axis_size(axis)
    behind, ahead = [x], [x]
    for k in range(size // 2):
        behind.append(shift(behind[-1], axis, 1))
        if k < size - size // 2 - 1:
            ahead.append(shift(ahead[-1], axis, -1))
    return behind + ahead[1:]


def ring_reduce(blocks, axis):
    size = lax.axis_size(axis)
    half = size // 2
    behind, ahead = blocks[1 : half + 1], blocks[half + 1 :]
    down, up = behind[-1], ahead[-1]
    for k in range(half):
        down = shift(down, axis, -1)
        if k < half - 1:
            down = (down.astype(f32) + behind[half - 2 - k].astype(f32)).astype(bf16)
        if k < half - 1:
            up = shift(up, axis, 1)
            if k < half - 2:
                up = (up.astype(f32) + ahead[half - 3 - k].astype(f32)).astype(bf16)
    return blocks[0].astype(f32) + down.astype(f32) + up.astype(f32)


def group_kernel(gate_ref, up_ref, down_ref, x_ref, kept_ref, out_ref, first_ref):
    del kept_ref
    groups, rows, width = x_ref.shape
    part = gate_ref.shape[-1]

    @pl.when(pl.program_id(0) == 0)
    def _():
        first_ref[:, :part] = gate_ref[0]
        first_ref[:, part:] = up_ref[0]

    x = x_ref[...].reshape(groups * rows, width)
    hidden = jnp.dot(x, first_ref[...], preferred_element_type=f32)
    act = (silu(hidden[:, :part]) * hidden[:, part:]).astype(bf16)
    total = jnp.dot(act, down_ref[0], preferred_element_type=f32)
    out_ref[...] = total.astype(bf16).reshape(out_ref.shape)


def grouped_mlp(x, gate, up, down, which, buffer):
    members, rows, model_width = x.shape
    part = gate.shape[2]
    groups = 4
    block = pl.BlockSpec((groups, rows, model_width), lambda t: (t, 0, 0))
    wide = pl.BlockSpec((1, model_width, part), lambda t: (which, 0, 0))
    return pl.pallas_call(
        group_kernel,
        grid=(members // groups,),
        in_specs=[
            wide,
            wide,
            pl.BlockSpec((1, part, model_width), lambda t: (which, 0, 0)),
            block,
            pl.BlockSpec(memory_space=pl.ANY),
        ],
        out_specs=block,
        out_shape=jax.ShapeDtypeStruct(buffer.shape, bf16),
        scratch_shapes=[pltpu.VMEM((model_width, 2 * part), bf16)],
        input_output_aliases={4: 0},
        compiler_params=pltpu.CompilerParams(vmem_limit_bytes=40 * 2**20),
    )(gate, up, down, x, buffer)


def masks():
    row = lax.broadcasted_iota(jnp.int32, (BLOCK, BLOCK), 0)
    column = lax.broadcasted_iota(jnp.int32, (BLOCK, BLOCK), 1)
    return row == column, row >= column


def upright(line, same):
    return jnp.sum(jnp.where(same, line, 0.0), axis=1, keepdims=True)


def advance(state, keys, values, line, column):
    end = line[:, BLOCK - 1 :]
    decayed = (keys.astype(f32) * jnp.exp(end - column)).astype(bf16)
    update = lax.dot_general(
        decayed, values, (((0,), (0,)), ((), ())), preferred_element_type=f32
    )
    return jnp.exp(end) * state + update


def state_kernel(q_ref, k_ref, v_ref, cos_ref, sin_ref, line_ref, qt_ref, kt_ref, out_ref, state_ref, log_ref):
    @pl.when(pl.program_id(0) == 0)
    def _():
        state_ref[...] = jnp.zeros_like(state_ref)
        log_ref[...] = jnp.zeros_like(log_ref)

    cosine, sine = cos_ref[...], sin_ref[...]
    half = q_ref.shape[1] // 2
    q, k = q_ref[...].astype(f32), k_ref[...].astype(f32)
    qt_ref[...] = (q * cosine + pltpu.roll(q, half, 1) * sine).astype(bf16)
    keys = (k * cosine + pltpu.roll(k, half, 1) * sine).astype(bf16)
    kt_ref[...] = keys
    line = line_ref[0]
    same, _ = masks()
    state_ref[...] = advance(state_ref[...], keys, v_ref[...], line, upright(line, same))
    log_ref[...] = log_ref[...] + line[:, BLOCK - 1 :]

    @pl.when(pl.program_id(0) == pl.num_programs(0) - 1)
    def _():
        rows = state_ref.shape[0]
        total = log_ref[...]
        high = total.astype(bf16).astype(f32)
        mark = lax.broadcasted_iota(jnp.int32, total.shape, 0)
        extra = jnp.where(mark == 0, high, jnp.where(mark == 1, total - high, 0.0))
        out_ref[:rows] = state_ref[...].astype(bf16)
        out_ref[rows:] = extra.astype(bf16)


def mixer_kernel(
    place_ref, pieces_ref, q_ref, k_ref, v_ref, gate_ref, line_ref, weight_ref, out_ref, state_ref, mixed_ref
):
    rows = state_ref.shape[0]
    strip = pl.program_id(1)

    @pl.when((pl.program_id(0) == 0) & (strip == 0))
    def _():
        state_ref[...] = jnp.zeros_like(state_ref)

        def enter(k, _):
            log = pieces_ref[k, rows : rows + 16, :].astype(f32)
            decay = jnp.exp(log[0:1, :] + log[1:2, :])
            state_ref[...] = decay * state_ref[...] + pieces_ref[k, :rows, :].astype(f32)
            return 0

        lax.fori_loop(0, place_ref[0], enter, 0)

    @pl.when(strip == 0)
    def _():
        queries, keys, values = q_ref[...], k_ref[...], v_ref[...]
        line = line_ref[0]
        same, lower = masks()
        column = upright(line, same)
        scores = lax.dot_general(
            queries, keys, (((1,), (1,)), ((), ())), preferred_element_type=f32
        )
        spread = jnp.where(lower, column - line, 0.0)
        weights = jnp.where(lower, scores * jnp.exp(spread), 0.0).astype(bf16)
        state = state_ref[...]
        retained = jnp.dot(weights, values, preferred_element_type=f32)
        retained = retained + jnp.dot(
            (queries.astype(f32) * jnp.exp(column)).astype(bf16),
            state.astype(bf16),
            preferred_element_type=f32,
        )
        state_ref[...] = advance(state, keys, values, line, column)
        mean = jnp.mean(retained * retained, axis=1, keepdims=True)
        gated = (silu(gate_ref[...].astype(f32)) * (retained * lax.rsqrt(mean + epsilon))).astype(bf16)
        mixed = jnp.dot(gated, weight_ref[...], preferred_element_type=f32)
        mixed_ref[...] = mixed.astype(bf16)

    for k in range(BLOCK // 2 // STRIP):

        @pl.when(strip == k)
        def _():
            for half in range(2):
                first = half * (BLOCK // 2) + k * STRIP
                out_ref[half] = mixed_ref[first : first + STRIP]


def own_state(query_rows, key_rows, value_rows, log_decay):
    tokens, key_width = query_rows.shape
    value_width = value_rows.shape[1]
    count = tokens // BLOCK
    start = lax.axis_index(EP) * tokens
    position = (start + jnp.arange(tokens, dtype=jnp.int32)).astype(f32)
    half_width = key_width // 2
    entry = jnp.arange(key_width)
    inverse = turn_base ** (-(entry % half_width).astype(f32) / half_width)
    angles = position[:, None] * inverse[None, :]
    cosine = jnp.cos(angles)
    sine = jnp.where(entry < half_width, -1.0, 1.0) * jnp.sin(angles)
    order = jnp.arange(BLOCK)
    upper = (order[:, None] <= order[None, :]).astype(f32)
    running = jnp.dot(log_decay.reshape(count, BLOCK), upper, precision=lax.Precision.HIGHEST)
    running = running.reshape(count, 1, BLOCK)

    def rows_of(width):
        return pl.BlockSpec((BLOCK, width), lambda n, *_: (n, 0))

    line = pl.BlockSpec((1, 1, BLOCK), lambda n, *_: (n, 0, 0))
    queries, keys, piece = pl.pallas_call(
        state_kernel,
        grid=(count,),
        in_specs=[rows_of(key_width)] * 2 + [rows_of(value_width)] + [rows_of(key_width)] * 2 + [line],
        out_specs=[
            rows_of(key_width),
            rows_of(key_width),
            pl.BlockSpec((key_width + 16, value_width), lambda n: (0, 0)),
        ],
        out_shape=[
            jax.ShapeDtypeStruct((tokens, key_width), bf16),
            jax.ShapeDtypeStruct((tokens, key_width), bf16),
            jax.ShapeDtypeStruct((key_width + 16, value_width), bf16),
        ],
        scratch_shapes=[
            pltpu.VMEM((key_width, value_width), f32),
            pltpu.VMEM((16, value_width), f32),
        ],
    )(query_rows, key_rows, value_rows, cosine, sine, running)
    return queries, keys, running, piece


def retention(
    queries, keys, running, pieces, value_rows, gate_rows, out_weight, rows_before
):
    tokens, key_width = queries.shape
    value_width = value_rows.shape[1]
    model_width = out_weight.shape[1]
    count = tokens // BLOCK
    members = lax.axis_size(TP)

    def rows_of(width):
        return pl.BlockSpec((BLOCK, width), lambda n, *_: (n, 0))

    line = pl.BlockSpec((1, 1, BLOCK), lambda n, *_: (n, 0, 0))
    where = jnp.reshape(lax.axis_index(EP), (1,)).astype(jnp.int32)
    strips = BLOCK // 2 // STRIP
    return pl.pallas_call(
        mixer_kernel,
        grid_spec=pltpu.PrefetchScalarGridSpec(
            num_scalar_prefetch=1,
            grid=(count, strips),
            in_specs=[
                pl.BlockSpec(pieces.shape, lambda n, *_: (0, 0, 0)),
                rows_of(key_width),
                rows_of(key_width),
                rows_of(value_width),
                rows_of(value_width),
                line,
                pl.BlockSpec(out_weight.shape, lambda n, *_: (0, 0)),
            ],
            out_specs=pl.BlockSpec(
                (2, STRIP, model_width), lambda n, k, *_: (n, rows_before // STRIP + k, 0)
            ),
            scratch_shapes=[
                pltpu.VMEM((key_width, value_width), f32),
                pltpu.VMEM((BLOCK, model_width), bf16),
            ],
        ),
        out_shape=pltpu.HBM((members, rows_before + tokens // members, model_width), bf16),
        compiler_params=pltpu.CompilerParams(vmem_limit_bytes=40 * 2**20),
    )(where, pieces, queries, keys, value_rows, gate_rows, running, out_weight)


def local(
    query_rows,
    key_rows,
    value_rows,
    gate_rows,
    log_decay,
    out_weight,
    channel_input,
    norm_gain,
    routes,
    route_weight,
    expert_gate,
    expert_up,
    expert_down,
    shared_gate,
    shared_up,
    shared_down,
):
    tokens_here, topk = routes.shape
    model_width = channel_input.shape[1]
    experts_here = expert_gate.shape[0]
    ep_count, levels = lax.axis_size(EP), lax.axis_size("z")
    experts_all = ep_count * experts_here
    picks = tokens_here * topk
    capacity = picks // experts_all + max(2, picks // (3 * experts_all))
    experts = (expert_gate, expert_up, expert_down)

    widened = channel_input.astype(f32)
    normed = (
        widened * lax.rsqrt(jnp.mean(widened * widened, axis=-1, keepdims=True) + epsilon) * norm_gain
    ).astype(bf16)
    flat = routes.reshape(-1)
    order = jnp.arange(picks, dtype=jnp.int32)
    same = (flat[:, None] == flat[None, :]) & (order[None, :] < order[:, None])
    rank = jnp.sum(same.astype(jnp.int32), axis=1).reshape(tokens_here, topk)
    slots = routes * capacity + rank
    meta = jnp.concatenate([slots.astype(bf16), route_weight.astype(bf16)], axis=1)
    meta = jnp.pad(meta, ((0, 0), (0, LANES - 2 * topk)))

    padded = jnp.where(routes % experts_here == 0, routes // experts_here * SLOTS + rank, -1)
    spots = jnp.arange(ep_count * SLOTS, dtype=jnp.int32)
    fetch = [(spots[:, None] == padded[None, :, k]).astype(bf16) for k in range(topk)]
    sent = jnp.dot(sum(fetch), normed, preferred_element_type=f32).astype(bf16)
    sent = sent.reshape(ep_count, SLOTS, model_width)
    arrived = lax.all_to_all(sent, EP, split_axis=0, concat_axis=0, tiled=True)
    arrived = jnp.transpose(arrived[:, :capacity], (1, 0, 2)).reshape(1, -1, model_width)
    gathered = lax.all_gather(arrived, TP, axis=0, tiled=True)

    own = jnp.concatenate([normed, meta], axis=1)
    queries, keys, running, piece = own_state(query_rows, key_rows, value_rows, log_decay)
    piece = jnp.broadcast_to(piece, (ep_count,) + piece.shape)
    pieces = lax.all_to_all(piece, EP, split_axis=0, concat_axis=0, tiled=True)
    rows = jnp.concatenate(ring_gather(own, "z"), axis=0)
    rows, pieces = lax.optimization_barrier((rows, pieces))
    placed = [
        place(rows, e, experts_here, capacity, levels, ep_count) for e in range(1, experts_here)
    ]
    placed, pieces = lax.optimization_barrier((placed, pieces))
    exchanged = []
    for sent in placed:
        sent = sent.reshape(ep_count, levels * capacity, model_width)
        arrived = lax.all_to_all(sent, EP, split_axis=0, concat_axis=0, tiled=True)
        exchanged.append(arrived.reshape(-1, model_width))

    buffer = retention(
        queries, keys, running, pieces, value_rows, gate_rows, out_weight, gathered.shape[1]
    )
    buffer = grouped_mlp(gathered, *experts, 0, buffer)
    summed = lax.psum_scatter(buffer, TP, scatter_dimension=0, tiled=True)[0]
    mixer = summed[gathered.shape[1] :]
    exchanged, _ = lax.optimization_barrier((exchanged, buffer))

    results = []
    for e, arrived in enumerate(exchanged, 1):
        other = gated_mlp(swap(arrived), *experts, e)
        both = gated_mlp(arrived, *experts, e, (swap(other),))
        both = both.reshape(ep_count, levels * capacity, model_width)
        back = lax.all_to_all(both, EP, split_axis=0, concat_axis=0, tiled=True)
        results.append(back.reshape(-1, model_width))

    shared = (shared_gate[None], shared_up[None], shared_down[None], 0)
    other = gated_mlp(swap(rows), *shared)
    total = gated_mlp(rows, *shared, (swap(other),))
    for e in range(1, experts_here):
        kind = bf16 if e == experts_here - 1 else f32
        total = collect(rows, results[e - 1], [total], e, experts_here, capacity, levels, kind)
    parts = [total[k * tokens_here : (k + 1) * tokens_here] for k in range(levels)]
    channel = ring_reduce(parts, "z")

    back = summed[: gathered.shape[1]].reshape(capacity, ep_count, model_width)
    back = jnp.pad(jnp.transpose(back, (1, 0, 2)), ((0, 0), (0, SLOTS - capacity), (0, 0)))
    returned = lax.all_to_all(back, EP, split_axis=0, concat_axis=0, tiled=True)
    returned = returned.reshape(-1, model_width)
    for k in range(topk):
        picked = jnp.dot(fetch[k].T, returned, preferred_element_type=f32)
        channel = channel + route_weight[:, k : k + 1] * picked
    return (mixer, channel.astype(bf16))


def solution(mesh):
    cores = 2
    split = Mesh(
        mesh.devices.reshape(4, 4, mesh.shape["tp"] // cores, cores), EP_TP
    )
    return jax.shard_map(
        local,
        mesh=split,
        in_specs=(
            P(EP, TP),
            P(EP, TP),
            P(EP, TP),
            P(EP, TP),
            P(TP, EP),
            P(TP, None),
            P(EP_TP, None),
            P(),
            P(EP_TP, None),
            P(EP_TP, None),
            P(EP, None, TP),
            P(EP, None, TP),
            P(EP, TP, None),
            P(None, TP),
            P(None, TP),
            P(TP, None),
        ),
        out_specs=(P(EP_TP, None), P(EP_TP, None)),
        check_vma=False,
    )
```

```python
import functools

import jax
import jax.numpy as jnp
from jax import lax
from jax.experimental import pallas as pl
from jax.experimental.pallas import tpu as pltpu
from jax.sharding import Mesh
from jax.sharding import PartitionSpec as P


BLOCK = 128
EP = ("ep_0", "ep_1")
TP = ("z", "core")
EP_TP = EP + TP
LANES = 128
SLOTS = 8

epsilon = 1e-06
turn_base = 10000.0
bf16 = jnp.bfloat16
f32 = jnp.float32


def silu(v):
    return v / (1.0 + jnp.exp(-v))


def hidden_kernel(gate_ref, up_ref, down_ref, x_ref, *refs):
    held, (out_ref, first_ref) = refs[:-2], refs[-2:]
    part = gate_ref.shape[-1]

    @pl.when(pl.program_id(0) == 0)
    def _():
        first_ref[:, :part] = gate_ref[0]
        first_ref[:, part:] = up_ref[0]

    hidden = jnp.dot(x_ref[...], first_ref[...], preferred_element_type=f32)
    act = (silu(hidden[:, :part]) * hidden[:, part:]).astype(bf16)
    total = jnp.dot(act, down_ref[0], preferred_element_type=f32)
    for ref in held:
        total = total + ref[...].astype(f32)
    out_ref[...] = total.astype(bf16)


def gated_mlp(x, gate, up, down, which, held=()):
    rows = x.shape[0]
    model_width, part = gate.shape[1:]
    step = rows // 2
    block = pl.BlockSpec((step, model_width), lambda i: (i, 0))
    wide = pl.BlockSpec((1, model_width, part), lambda i: (which, 0, 0))
    return pl.pallas_call(
        hidden_kernel,
        grid=(rows // step,),
        in_specs=[
            wide,
            wide,
            pl.BlockSpec((1, part, model_width), lambda i: (which, 0, 0)),
            block,
        ]
        + [block] * len(held),
        out_specs=block,
        out_shape=pltpu.HBM((rows, model_width), bf16),
        scratch_shapes=[pltpu.VMEM((model_width, 2 * part), bf16)],
        compiler_params=pltpu.CompilerParams(vmem_limit_bytes=40 * 2**20),
    )(gate, up, down, x, *held)


def column_codes(shape, expert, experts_here, capacity, blocks):
    column = lax.broadcasted_iota(jnp.int32, shape, 1)
    block_rows = blocks * capacity
    target, rest = column // block_rows, column % block_rows
    block, rank = rest // capacity, rest % capacity
    return target * (experts_here * capacity) + expert * capacity + rank, block


def place_kernel(expert, experts_here, capacity, blocks, x_ref, meta_ref, out_ref, hits_ref):
    @pl.when(pl.program_id(0) == 0)
    def _():
        meta = meta_ref[...].astype(f32).astype(jnp.int32)
        shape = hits_ref.shape
        code, block = column_codes(shape, expert, experts_here, capacity, blocks)
        row = lax.broadcasted_iota(jnp.int32, shape, 0) // (shape[0] // blocks)
        hit = ((meta[:, 0:1] == code) | (meta[:, 1:2] == code)) & (row == block)
        hits_ref[...] = jnp.where(hit, 1.0, 0.0).astype(bf16)

    out_ref[...] = lax.dot_general(
        hits_ref[...], x_ref[...], (((0,), (0,)), ((), ())), preferred_element_type=f32
    ).astype(bf16)


def place(rows, expert, experts_here, capacity, blocks, targets):
    count, width = rows.shape
    model_width = width - LANES
    step = 512
    out_rows = targets * blocks * capacity
    return pl.pallas_call(
        functools.partial(place_kernel, expert, experts_here, capacity, blocks),
        grid=(model_width // step,),
        in_specs=[
            pl.BlockSpec((count, step), lambda i: (0, i)),
            pl.BlockSpec((count, LANES), lambda i: (0, model_width // LANES)),
        ],
        out_specs=pl.BlockSpec((out_rows, step), lambda i: (0, i)),
        out_shape=pltpu.HBM((out_rows, model_width), bf16),
        scratch_shapes=[pltpu.VMEM((count, out_rows), bf16)],
        compiler_params=pltpu.CompilerParams(vmem_limit_bytes=40 * 2**20),
    )(rows, rows)


def collect_kernel(expert, experts_here, capacity, blocks, meta_ref, back_ref, *refs):
    held, (out_ref, share_ref) = refs[:-2], refs[-2:]

    @pl.when(pl.program_id(0) == 0)
    def _():
        meta = meta_ref[...].astype(f32)
        slot = meta.astype(jnp.int32)
        shape = share_ref.shape
        code, block = column_codes(shape, expert, experts_here, capacity, blocks)
        here = lax.broadcasted_iota(jnp.int32, shape, 0) // (shape[0] // blocks) == block
        first = jnp.where((slot[:, 0:1] == code) & here, meta[:, 2:3], 0.0)
        second = jnp.where((slot[:, 1:2] == code) & here, meta[:, 3:4], 0.0)
        share_ref[...] = (first + second).astype(bf16)

    total = jnp.dot(share_ref[...], back_ref[...], preferred_element_type=f32)
    for ref in held:
        total = total + ref[...].astype(f32)
    out_ref[...] = total.astype(out_ref.dtype)


def collect(rows, back, held, expert, experts_here, capacity, blocks, kind):
    count, width = rows.shape
    model_width = width - LANES
    step = 512
    return pl.pallas_call(
        functools.partial(collect_kernel, expert, experts_here, capacity, blocks),
        grid=(model_width // step,),
        in_specs=[
            pl.BlockSpec((count, LANES), lambda i: (0, model_width // LANES)),
            pl.BlockSpec((back.shape[0], step), lambda i: (0, i)),
        ]
        + [pl.BlockSpec((count, step), lambda i: (0, i))] * len(held),
        out_specs=pl.BlockSpec((count, step), lambda i: (0, i)),
        out_shape=jax.ShapeDtypeStruct((count, model_width), kind),
        scratch_shapes=[pltpu.VMEM((count, back.shape[0]), bf16)],
        compiler_params=pltpu.CompilerParams(vmem_limit_bytes=40 * 2**20),
    )(rows, back, *held)


def shift(x, axis, by):
    size = lax.axis_size(axis)
    return lax.ppermute(x, axis, [(i, (i + by) % size) for i in range(size)])


def swap(x):
    return lax.ppermute(x, "core", [(0, 1), (1, 0)])


def ring_gather(x, axis):
    size = lax.axis_size(axis)
    behind, ahead = [x], [x]
    for k in range(size // 2):
        behind.append(shift(behind[-1], axis, 1))
        if k < size - size // 2 - 1:
            ahead.append(shift(ahead[-1], axis, -1))
    return behind + ahead[1:]


def ring_reduce(blocks, axis):
    size = lax.axis_size(axis)
    half = size // 2
    behind, ahead = blocks[1 : half + 1], blocks[half + 1 :]
    down, up = behind[-1], ahead[-1]
    for k in range(half):
        down = shift(down, axis, -1)
        if k < half - 1:
            down = (down.astype(f32) + behind[half - 2 - k].astype(f32)).astype(bf16)
        if k < half - 1:
            up = shift(up, axis, 1)
            if k < half - 2:
                up = (up.astype(f32) + ahead[half - 3 - k].astype(f32)).astype(bf16)
    return blocks[0].astype(f32) + down.astype(f32) + up.astype(f32)


def group_kernel(gate_ref, up_ref, down_ref, x_ref, kept_ref, out_ref, first_ref):
    del kept_ref
    groups, rows, width = x_ref.shape
    part = gate_ref.shape[-1]

    @pl.when(pl.program_id(0) == 0)
    def _():
        first_ref[:, :part] = gate_ref[0]
        first_ref[:, part:] = up_ref[0]

    x = x_ref[...].reshape(groups * rows, width)
    hidden = jnp.dot(x, first_ref[...], preferred_element_type=f32)
    act = (silu(hidden[:, :part]) * hidden[:, part:]).astype(bf16)
    total = jnp.dot(act, down_ref[0], preferred_element_type=f32)
    out_ref[...] = total.astype(bf16).reshape(out_ref.shape)


def grouped_mlp(x, gate, up, down, which, buffer):
    members, rows, model_width = x.shape
    part = gate.shape[2]
    groups = 4
    block = pl.BlockSpec((groups, rows, model_width), lambda t: (t, 0, 0))
    wide = pl.BlockSpec((1, model_width, part), lambda t: (which, 0, 0))
    return pl.pallas_call(
        group_kernel,
        grid=(members // groups,),
        in_specs=[
            wide,
            wide,
            pl.BlockSpec((1, part, model_width), lambda t: (which, 0, 0)),
            block,
            pl.BlockSpec(memory_space=pl.ANY),
        ],
        out_specs=block,
        out_shape=jax.ShapeDtypeStruct(buffer.shape, bf16),
        scratch_shapes=[pltpu.VMEM((model_width, 2 * part), bf16)],
        input_output_aliases={4: 0},
        compiler_params=pltpu.CompilerParams(vmem_limit_bytes=40 * 2**20),
    )(gate, up, down, x, buffer)


def masks():
    row = lax.broadcasted_iota(jnp.int32, (BLOCK, BLOCK), 0)
    column = lax.broadcasted_iota(jnp.int32, (BLOCK, BLOCK), 1)
    return row == column, row >= column


def upright(line, same):
    return jnp.sum(jnp.where(same, line, 0.0), axis=1, keepdims=True)


def advance(state, keys, values, line, column):
    end = line[:, BLOCK - 1 :]
    decayed = (keys.astype(f32) * jnp.exp(end - column)).astype(bf16)
    update = lax.dot_general(
        decayed, values, (((0,), (0,)), ((), ())), preferred_element_type=f32
    )
    return jnp.exp(end) * state + update


def state_kernel(q_ref, k_ref, v_ref, cos_ref, sin_ref, line_ref, qt_ref, kt_ref, out_ref, state_ref, log_ref):
    @pl.when(pl.program_id(0) == 0)
    def _():
        state_ref[...] = jnp.zeros_like(state_ref)
        log_ref[...] = jnp.zeros_like(log_ref)

    cosine, sine = cos_ref[...], sin_ref[...]
    half = q_ref.shape[1] // 2
    q, k = q_ref[...].astype(f32), k_ref[...].astype(f32)
    qt_ref[...] = (q * cosine + pltpu.roll(q, half, 1) * sine).astype(bf16)
    keys = (k * cosine + pltpu.roll(k, half, 1) * sine).astype(bf16)
    kt_ref[...] = keys
    line = line_ref[0]
    same, _ = masks()
    state_ref[...] = advance(state_ref[...], keys, v_ref[...], line, upright(line, same))
    log_ref[...] = log_ref[...] + line[:, BLOCK - 1 :]

    @pl.when(pl.program_id(0) == pl.num_programs(0) - 1)
    def _():
        rows = state_ref.shape[0]
        total = log_ref[...]
        high = total.astype(bf16).astype(f32)
        mark = lax.broadcasted_iota(jnp.int32, total.shape, 0)
        extra = jnp.where(mark == 0, high, jnp.where(mark == 1, total - high, 0.0))
        out_ref[:rows] = state_ref[...].astype(bf16)
        out_ref[rows:] = extra.astype(bf16)


def mixer_kernel(
    place_ref, pieces_ref, q_ref, k_ref, v_ref, gate_ref, line_ref, weight_ref, out_ref, state_ref
):
    rows = state_ref.shape[0]

    @pl.when(pl.program_id(0) == 0)
    def _():
        state_ref[...] = jnp.zeros_like(state_ref)

        def enter(k, _):
            log = pieces_ref[k, rows : rows + 16, :].astype(f32)
            decay = jnp.exp(log[0:1, :] + log[1:2, :])
            state_ref[...] = decay * state_ref[...] + pieces_ref[k, :rows, :].astype(f32)
            return 0

        lax.fori_loop(0, place_ref[0], enter, 0)

    queries, keys, values = q_ref[...], k_ref[...], v_ref[...]
    line = line_ref[0]
    same, lower = masks()
    column = upright(line, same)
    scores = lax.dot_general(
        queries, keys, (((1,), (1,)), ((), ())), preferred_element_type=f32
    )
    spread = jnp.where(lower, column - line, 0.0)
    weights = jnp.where(lower, scores * jnp.exp(spread), 0.0).astype(bf16)
    state = state_ref[...]
    retained = jnp.dot(weights, values, preferred_element_type=f32)
    retained = retained + jnp.dot(
        (queries.astype(f32) * jnp.exp(column)).astype(bf16),
        state.astype(bf16),
        preferred_element_type=f32,
    )
    state_ref[...] = advance(state, keys, values, line, column)
    mean = jnp.mean(retained * retained, axis=1, keepdims=True)
    gated = (silu(gate_ref[...].astype(f32)) * (retained * lax.rsqrt(mean + epsilon))).astype(bf16)
    mixed = jnp.dot(gated, weight_ref[...], preferred_element_type=f32)
    out_ref[...] = mixed.astype(bf16).reshape(out_ref.shape)


def own_state(query_rows, key_rows, value_rows, log_decay):
    tokens, key_width = query_rows.shape
    value_width = value_rows.shape[1]
    count = tokens // BLOCK
    start = lax.axis_index(EP) * tokens
    position = (start + jnp.arange(tokens, dtype=jnp.int32)).astype(f32)
    half_width = key_width // 2
    entry = jnp.arange(key_width)
    inverse = turn_base ** (-(entry % half_width).astype(f32) / half_width)
    angles = position[:, None] * inverse[None, :]
    cosine = jnp.cos(angles)
    sine = jnp.where(entry < half_width, -1.0, 1.0) * jnp.sin(angles)
    order = jnp.arange(BLOCK)
    upper = (order[:, None] <= order[None, :]).astype(f32)
    running = jnp.dot(log_decay.reshape(count, BLOCK), upper, precision=lax.Precision.HIGHEST)
    running = running.reshape(count, 1, BLOCK)

    def rows_of(width):
        return pl.BlockSpec((BLOCK, width), lambda n, *_: (n, 0))

    line = pl.BlockSpec((1, 1, BLOCK), lambda n, *_: (n, 0, 0))
    queries, keys, piece = pl.pallas_call(
        state_kernel,
        grid=(count,),
        in_specs=[rows_of(key_width)] * 2 + [rows_of(value_width)] + [rows_of(key_width)] * 2 + [line],
        out_specs=[
            rows_of(key_width),
            rows_of(key_width),
            pl.BlockSpec((key_width + 16, value_width), lambda n: (0, 0)),
        ],
        out_shape=[
            jax.ShapeDtypeStruct((tokens, key_width), bf16),
            jax.ShapeDtypeStruct((tokens, key_width), bf16),
            jax.ShapeDtypeStruct((key_width + 16, value_width), bf16),
        ],
        scratch_shapes=[
            pltpu.VMEM((key_width, value_width), f32),
            pltpu.VMEM((16, value_width), f32),
        ],
    )(query_rows, key_rows, value_rows, cosine, sine, running)
    return queries, keys, running, piece


def retention(
    queries, keys, running, pieces, value_rows, gate_rows, out_weight, rows_before
):
    tokens, key_width = queries.shape
    value_width = value_rows.shape[1]
    model_width = out_weight.shape[1]
    count = tokens // BLOCK
    members = lax.axis_size(TP)

    def rows_of(width):
        return pl.BlockSpec((BLOCK, width), lambda n, *_: (n, 0))

    line = pl.BlockSpec((1, 1, BLOCK), lambda n, *_: (n, 0, 0))
    where = jnp.reshape(lax.axis_index(EP), (1,)).astype(jnp.int32)
    return pl.pallas_call(
        mixer_kernel,
        grid_spec=pltpu.PrefetchScalarGridSpec(
            num_scalar_prefetch=1,
            grid=(count,),
            in_specs=[
                pl.BlockSpec(pieces.shape, lambda n, *_: (0, 0, 0)),
                rows_of(key_width),
                rows_of(key_width),
                rows_of(value_width),
                rows_of(value_width),
                line,
                pl.BlockSpec(out_weight.shape, lambda n, *_: (0, 0)),
            ],
            out_specs=pl.BlockSpec(
                (pl.Element(2), pl.Element(BLOCK // 2), pl.Element(model_width)),
                lambda n, *_: (2 * n, rows_before, 0),
            ),
            scratch_shapes=[pltpu.VMEM((key_width, value_width), f32)],
        ),
        out_shape=pltpu.HBM((members, rows_before + tokens // members, model_width), bf16),
        compiler_params=pltpu.CompilerParams(vmem_limit_bytes=40 * 2**20),
    )(where, pieces, queries, keys, value_rows, gate_rows, running, out_weight)


def local(
    query_rows,
    key_rows,
    value_rows,
    gate_rows,
    log_decay,
    out_weight,
    channel_input,
    norm_gain,
    routes,
    route_weight,
    expert_gate,
    expert_up,
    expert_down,
    shared_gate,
    shared_up,
    shared_down,
):
    tokens_here, topk = routes.shape
    model_width = channel_input.shape[1]
    experts_here = expert_gate.shape[0]
    ep_count, levels = lax.axis_size(EP), lax.axis_size("z")
    experts_all = ep_count * experts_here
    picks = tokens_here * topk
    capacity = picks // experts_all + max(2, picks // (3 * experts_all))
    experts = (expert_gate, expert_up, expert_down)

    widened = channel_input.astype(f32)
    normed = (
        widened * lax.rsqrt(jnp.mean(widened * widened, axis=-1, keepdims=True) + epsilon) * norm_gain
    ).astype(bf16)
    flat = routes.reshape(-1)
    order = jnp.arange(picks, dtype=jnp.int32)
    same = (flat[:, None] == flat[None, :]) & (order[None, :] < order[:, None])
    rank = jnp.sum(same.astype(jnp.int32), axis=1).reshape(tokens_here, topk)
    slots = routes * capacity + rank
    meta = jnp.concatenate([slots.astype(bf16), route_weight.astype(bf16)], axis=1)
    meta = jnp.pad(meta, ((0, 0), (0, LANES - 2 * topk)))

    padded = jnp.where(routes % experts_here == 0, routes // experts_here * SLOTS + rank, -1)
    spots = jnp.arange(ep_count * SLOTS, dtype=jnp.int32)
    fetch = [(spots[:, None] == padded[None, :, k]).astype(bf16) for k in range(topk)]
    sent = jnp.dot(sum(fetch), normed, preferred_element_type=f32).astype(bf16)
    sent = sent.reshape(ep_count, SLOTS, model_width)
    arrived = lax.all_to_all(sent, EP, split_axis=0, concat_axis=0, tiled=True)
    arrived = jnp.transpose(arrived[:, :capacity], (1, 0, 2)).reshape(1, -1, model_width)

    own = jnp.concatenate([normed, meta], axis=1)
    queries, keys, running, piece = own_state(query_rows, key_rows, value_rows, log_decay)
    piece = jnp.broadcast_to(piece, (ep_count,) + piece.shape)
    pieces = lax.all_to_all(piece, EP, split_axis=0, concat_axis=0, tiled=True)
    blocks = ring_gather(own, "z")
    arrived, blocks[levels // 2 - 1] = lax.optimization_barrier((arrived, blocks[levels // 2 - 1]))
    gathered = lax.all_gather(arrived, TP, axis=0, tiled=True)
    rows = jnp.concatenate(blocks, axis=0)
    rows, pieces = lax.optimization_barrier((rows, pieces))
    placed = [
        place(rows, e, experts_here, capacity, levels, ep_count) for e in range(1, experts_here)
    ]
    placed, pieces = lax.optimization_barrier((placed, pieces))
    exchanged = []
    for sent in placed:
        sent = sent.reshape(ep_count, levels * capacity, model_width)
        arrived = lax.all_to_all(sent, EP, split_axis=0, concat_axis=0, tiled=True)
        exchanged.append(arrived.reshape(-1, model_width))

    buffer = retention(
        queries, keys, running, pieces, value_rows, gate_rows, out_weight, gathered.shape[1]
    )
    buffer = grouped_mlp(gathered, *experts, 0, buffer)
    summed = lax.psum_scatter(buffer, TP, scatter_dimension=0, tiled=True)[0]
    mixer = summed[gathered.shape[1] :]
    exchanged, _ = lax.optimization_barrier((exchanged, buffer))

    results = []
    for e, arrived in enumerate(exchanged, 1):
        other = gated_mlp(swap(arrived), *experts, e)
        both = gated_mlp(arrived, *experts, e, (swap(other),))
        both = both.reshape(ep_count, levels * capacity, model_width)
        back = lax.all_to_all(both, EP, split_axis=0, concat_axis=0, tiled=True)
        results.append(back.reshape(-1, model_width))

    shared = (shared_gate[None], shared_up[None], shared_down[None], 0)
    other = gated_mlp(swap(rows), *shared)
    total = gated_mlp(rows, *shared, (swap(other),))
    for e in range(1, experts_here):
        kind = bf16 if e == experts_here - 1 else f32
        total = collect(rows, results[e - 1], [total], e, experts_here, capacity, levels, kind)
    parts = [total[k * tokens_here : (k + 1) * tokens_here] for k in range(levels)]
    channel = ring_reduce(parts, "z")

    back = summed[: gathered.shape[1]].reshape(capacity, ep_count, model_width)
    back = jnp.pad(jnp.transpose(back, (1, 0, 2)), ((0, 0), (0, SLOTS - capacity), (0, 0)))
    returned = lax.all_to_all(back, EP, split_axis=0, concat_axis=0, tiled=True)
    returned = returned.reshape(-1, model_width)
    for k in range(topk):
        picked = jnp.dot(fetch[k].T, returned, preferred_element_type=f32)
        channel = channel + route_weight[:, k : k + 1] * picked
    return (mixer, channel.astype(bf16))


def solution(mesh):
    cores = 2
    split = Mesh(
        mesh.devices.reshape(4, 4, mesh.shape["tp"] // cores, cores), EP_TP
    )
    return jax.shard_map(
        local,
        mesh=split,
        in_specs=(
            P(EP, TP),
            P(EP, TP),
            P(EP, TP),
            P(EP, TP),
            P(TP, EP),
            P(TP, None),
            P(EP_TP, None),
            P(),
            P(EP_TP, None),
            P(EP_TP, None),
            P(EP, None, TP),
            P(EP, None, TP),
            P(EP, TP, None),
            P(None, TP),
            P(None, TP),
            P(TP, None),
        ),
        out_specs=(P(EP_TP, None), P(EP_TP, None)),
        check_vma=False,
    )
```

```python
import functools

import jax
import jax.numpy as jnp
from jax import lax
from jax.experimental import pallas as pl
from jax.experimental.pallas import tpu as pltpu
from jax.sharding import Mesh
from jax.sharding import PartitionSpec as P


BLOCK = 128
EP = ("ep_0", "ep_1")
TP = ("z", "core")
EP_TP = EP + TP
LANES = 128
SLOTS = 8

epsilon = 1e-06
turn_base = 10000.0
bf16 = jnp.bfloat16
f32 = jnp.float32


def silu(v):
    return v / (1.0 + jnp.exp(-v))


def hidden_kernel(gate_ref, up_ref, down_ref, x_ref, *refs):
    held, (out_ref, first_ref) = refs[:-2], refs[-2:]
    part = gate_ref.shape[-1]

    @pl.when(pl.program_id(0) == 0)
    def _():
        first_ref[:, :part] = gate_ref[0]
        first_ref[:, part:] = up_ref[0]

    hidden = jnp.dot(x_ref[...], first_ref[...], preferred_element_type=f32)
    act = (silu(hidden[:, :part]) * hidden[:, part:]).astype(bf16)
    total = jnp.dot(act, down_ref[0], preferred_element_type=f32)
    if not held:
        out_ref[...] = total.astype(bf16)
    for k, ref in enumerate(held):

        @pl.when(pl.program_id(0) == k)
        def _(ref=ref):
            out_ref[...] = (total + ref[...].astype(f32)).astype(bf16)


def gated_mlp(x, gate, up, down, which, held=(), parts=2):
    rows = x.shape[0]
    model_width, part = gate.shape[1:]
    step = rows // parts
    block = pl.BlockSpec((step, model_width), lambda i: (i, 0))
    wide = pl.BlockSpec((1, model_width, part), lambda i: (which, 0, 0))
    return pl.pallas_call(
        hidden_kernel,
        grid=(rows // step,),
        in_specs=[
            wide,
            wide,
            pl.BlockSpec((1, part, model_width), lambda i: (which, 0, 0)),
            block,
        ]
        + [pl.BlockSpec((step, model_width), lambda i: (0, 0))] * len(held),
        out_specs=block,
        out_shape=pltpu.HBM((rows, model_width), bf16),
        scratch_shapes=[pltpu.VMEM((model_width, 2 * part), bf16)],
        compiler_params=pltpu.CompilerParams(vmem_limit_bytes=40 * 2**20),
    )(gate, up, down, x, *held)


def column_codes(shape, expert, experts_here, capacity, blocks):
    column = lax.broadcasted_iota(jnp.int32, shape, 1)
    block_rows = blocks * capacity
    target, rest = column // block_rows, column % block_rows
    block, rank = rest // capacity, rest % capacity
    return target * (experts_here * capacity) + expert * capacity + rank, block


def place_kernel(expert, experts_here, capacity, blocks, x_ref, meta_ref, out_ref, hits_ref):
    @pl.when(pl.program_id(0) == 0)
    def _():
        meta = meta_ref[...].astype(f32).astype(jnp.int32)
        shape = hits_ref.shape
        code, block = column_codes(shape, expert, experts_here, capacity, blocks)
        row = lax.broadcasted_iota(jnp.int32, shape, 0) // (shape[0] // blocks)
        hit = ((meta[:, 0:1] == code) | (meta[:, 1:2] == code)) & (row == block)
        hits_ref[...] = jnp.where(hit, 1.0, 0.0).astype(bf16)

    out_ref[...] = lax.dot_general(
        hits_ref[...], x_ref[...], (((0,), (0,)), ((), ())), preferred_element_type=f32
    ).astype(bf16)


def place(rows, expert, experts_here, capacity, blocks, targets):
    count, width = rows.shape
    model_width = width - LANES
    step = 512
    out_rows = targets * blocks * capacity
    return pl.pallas_call(
        functools.partial(place_kernel, expert, experts_here, capacity, blocks),
        grid=(model_width // step,),
        in_specs=[
            pl.BlockSpec((count, step), lambda i: (0, i)),
            pl.BlockSpec((count, LANES), lambda i: (0, model_width // LANES)),
        ],
        out_specs=pl.BlockSpec((out_rows, step), lambda i: (0, i)),
        out_shape=pltpu.HBM((out_rows, model_width), bf16),
        scratch_shapes=[pltpu.VMEM((count, out_rows), bf16)],
        compiler_params=pltpu.CompilerParams(vmem_limit_bytes=40 * 2**20),
    )(rows, rows)


def collect_kernel(expert, experts_here, capacity, blocks, meta_ref, back_ref, *refs):
    held, (out_ref, share_ref) = refs[:-2], refs[-2:]

    @pl.when(pl.program_id(0) == 0)
    def _():
        meta = meta_ref[...].astype(f32)
        slot = meta.astype(jnp.int32)
        shape = share_ref.shape
        code, block = column_codes(shape, expert, experts_here, capacity, blocks)
        here = lax.broadcasted_iota(jnp.int32, shape, 0) // (shape[0] // blocks) == block
        first = jnp.where((slot[:, 0:1] == code) & here, meta[:, 2:3], 0.0)
        second = jnp.where((slot[:, 1:2] == code) & here, meta[:, 3:4], 0.0)
        share_ref[...] = (first + second).astype(bf16)

    total = jnp.dot(share_ref[...], back_ref[...], preferred_element_type=f32)
    for ref in held:
        total = total + ref[...].astype(f32)
    out_ref[...] = total.astype(out_ref.dtype)


def collect(rows, back, held, expert, experts_here, capacity, blocks, kind):
    count, width = rows.shape
    model_width = width - LANES
    step = 512
    return pl.pallas_call(
        functools.partial(collect_kernel, expert, experts_here, capacity, blocks),
        grid=(model_width // step,),
        in_specs=[
            pl.BlockSpec((count, LANES), lambda i: (0, model_width // LANES)),
            pl.BlockSpec((back.shape[0], step), lambda i: (0, i)),
        ]
        + [pl.BlockSpec((count, step), lambda i: (0, i))] * len(held),
        out_specs=pl.BlockSpec((count, step), lambda i: (0, i)),
        out_shape=jax.ShapeDtypeStruct((count, model_width), kind),
        scratch_shapes=[pltpu.VMEM((count, back.shape[0]), bf16)],
        compiler_params=pltpu.CompilerParams(vmem_limit_bytes=40 * 2**20),
    )(rows, back, *held)


def shift(x, axis, by):
    size = lax.axis_size(axis)
    return lax.ppermute(x, axis, [(i, (i + by) % size) for i in range(size)])


def swap(x):
    return lax.ppermute(x, "core", [(0, 1), (1, 0)])


def ring_gather(x, axis):
    size = lax.axis_size(axis)
    behind, ahead = [x], [x]
    for k in range(size // 2):
        behind.append(shift(behind[-1], axis, 1))
        if k < size - size // 2 - 1:
            ahead.append(shift(ahead[-1], axis, -1))
    return behind + ahead[1:]


def ring_reduce(blocks, axis):
    size = lax.axis_size(axis)
    half = size // 2
    behind, ahead = blocks[1 : half + 1], blocks[half + 1 :]
    down, up = behind[-1], ahead[-1]
    for k in range(half):
        down = shift(down, axis, -1)
        if k < half - 1:
            down = (down.astype(f32) + behind[half - 2 - k].astype(f32)).astype(bf16)
        if k < half - 1:
            up = shift(up, axis, 1)
            if k < half - 2:
                up = (up.astype(f32) + ahead[half - 3 - k].astype(f32)).astype(bf16)
    return blocks[0].astype(f32) + down.astype(f32) + up.astype(f32)


def group_kernel(gate_ref, up_ref, down_ref, x_ref, kept_ref, out_ref, first_ref):
    del kept_ref
    groups, rows, width = x_ref.shape
    part = gate_ref.shape[-1]

    @pl.when(pl.program_id(0) == 0)
    def _():
        first_ref[:, :part] = gate_ref[0]
        first_ref[:, part:] = up_ref[0]

    x = x_ref[...].reshape(groups * rows, width)
    hidden = jnp.dot(x, first_ref[...], preferred_element_type=f32)
    act = (silu(hidden[:, :part]) * hidden[:, part:]).astype(bf16)
    total = jnp.dot(act, down_ref[0], preferred_element_type=f32)
    out_ref[...] = total.astype(bf16).reshape(out_ref.shape)


def grouped_mlp(x, gate, up, down, which, buffer):
    members, rows, model_width = x.shape
    part = gate.shape[2]
    groups = 4
    block = pl.BlockSpec((groups, rows, model_width), lambda t: (t, 0, 0))
    wide = pl.BlockSpec((1, model_width, part), lambda t: (which, 0, 0))
    return pl.pallas_call(
        group_kernel,
        grid=(members // groups,),
        in_specs=[
            wide,
            wide,
            pl.BlockSpec((1, part, model_width), lambda t: (which, 0, 0)),
            block,
            pl.BlockSpec(memory_space=pl.ANY),
        ],
        out_specs=block,
        out_shape=jax.ShapeDtypeStruct(buffer.shape, bf16),
        scratch_shapes=[pltpu.VMEM((model_width, 2 * part), bf16)],
        input_output_aliases={4: 0},
        compiler_params=pltpu.CompilerParams(vmem_limit_bytes=40 * 2**20),
    )(gate, up, down, x, buffer)


def masks():
    row = lax.broadcasted_iota(jnp.int32, (BLOCK, BLOCK), 0)
    column = lax.broadcasted_iota(jnp.int32, (BLOCK, BLOCK), 1)
    return row == column, row >= column


def upright(line, same):
    return jnp.sum(jnp.where(same, line, 0.0), axis=1, keepdims=True)


def advance(state, keys, values, line, column):
    end = line[:, BLOCK - 1 :]
    decayed = (keys.astype(f32) * jnp.exp(end - column)).astype(bf16)
    update = lax.dot_general(
        decayed, values, (((0,), (0,)), ((), ())), preferred_element_type=f32
    )
    return jnp.exp(end) * state + update


def state_kernel(q_ref, k_ref, v_ref, cos_ref, sin_ref, line_ref, qt_ref, kt_ref, out_ref, state_ref, log_ref):
    @pl.when(pl.program_id(0) == 0)
    def _():
        state_ref[...] = jnp.zeros_like(state_ref)
        log_ref[...] = jnp.zeros_like(log_ref)

    cosine, sine = cos_ref[...], sin_ref[...]
    half = q_ref.shape[1] // 2
    q, k = q_ref[...].astype(f32), k_ref[...].astype(f32)
    qt_ref[...] = (q * cosine + pltpu.roll(q, half, 1) * sine).astype(bf16)
    keys = (k * cosine + pltpu.roll(k, half, 1) * sine).astype(bf16)
    kt_ref[...] = keys
    line = line_ref[0]
    same, _ = masks()
    state_ref[...] = advance(state_ref[...], keys, v_ref[...], line, upright(line, same))
    log_ref[...] = log_ref[...] + line[:, BLOCK - 1 :]

    @pl.when(pl.program_id(0) == pl.num_programs(0) - 1)
    def _():
        rows = state_ref.shape[0]
        total = log_ref[...]
        high = total.astype(bf16).astype(f32)
        mark = lax.broadcasted_iota(jnp.int32, total.shape, 0)
        extra = jnp.where(mark == 0, high, jnp.where(mark == 1, total - high, 0.0))
        out_ref[:rows] = state_ref[...].astype(bf16)
        out_ref[rows:] = extra.astype(bf16)


def mixer_kernel(
    place_ref, pieces_ref, q_ref, k_ref, v_ref, gate_ref, line_ref, weight_ref, out_ref, state_ref
):
    rows = state_ref.shape[0]

    @pl.when(pl.program_id(0) == 0)
    def _():
        state_ref[...] = jnp.zeros_like(state_ref)

        def enter(k, _):
            log = pieces_ref[k, rows : rows + 16, :].astype(f32)
            decay = jnp.exp(log[0:1, :] + log[1:2, :])
            state_ref[...] = decay * state_ref[...] + pieces_ref[k, :rows, :].astype(f32)
            return 0

        lax.fori_loop(0, place_ref[0], enter, 0)

    queries, keys, values = q_ref[...], k_ref[...], v_ref[...]
    line = line_ref[0]
    same, lower = masks()
    column = upright(line, same)
    scores = lax.dot_general(
        queries, keys, (((1,), (1,)), ((), ())), preferred_element_type=f32
    )
    spread = jnp.where(lower, column - line, 0.0)
    weights = jnp.where(lower, scores * jnp.exp(spread), 0.0).astype(bf16)
    state = state_ref[...]
    retained = jnp.dot(weights, values, preferred_element_type=f32)
    retained = retained + jnp.dot(
        (queries.astype(f32) * jnp.exp(column)).astype(bf16),
        state.astype(bf16),
        preferred_element_type=f32,
    )
    state_ref[...] = advance(state, keys, values, line, column)
    mean = jnp.mean(retained * retained, axis=1, keepdims=True)
    gated = (silu(gate_ref[...].astype(f32)) * (retained * lax.rsqrt(mean + epsilon))).astype(bf16)
    mixed = jnp.dot(gated, weight_ref[...], preferred_element_type=f32)
    out_ref[...] = mixed.astype(bf16).reshape(out_ref.shape)


def own_state(query_rows, key_rows, value_rows, log_decay):
    tokens, key_width = query_rows.shape
    value_width = value_rows.shape[1]
    count = tokens // BLOCK
    start = lax.axis_index(EP) * tokens
    position = (start + jnp.arange(tokens, dtype=jnp.int32)).astype(f32)
    half_width = key_width // 2
    entry = jnp.arange(key_width)
    inverse = turn_base ** (-(entry % half_width).astype(f32) / half_width)
    angles = position[:, None] * inverse[None, :]
    cosine = jnp.cos(angles)
    sine = jnp.where(entry < half_width, -1.0, 1.0) * jnp.sin(angles)
    order = jnp.arange(BLOCK)
    upper = (order[:, None] <= order[None, :]).astype(f32)
    running = jnp.dot(log_decay.reshape(count, BLOCK), upper, precision=lax.Precision.HIGHEST)
    running = running.reshape(count, 1, BLOCK)

    def rows_of(width):
        return pl.BlockSpec((BLOCK, width), lambda n, *_: (n, 0))

    line = pl.BlockSpec((1, 1, BLOCK), lambda n, *_: (n, 0, 0))
    queries, keys, piece = pl.pallas_call(
        state_kernel,
        grid=(count,),
        in_specs=[rows_of(key_width)] * 2 + [rows_of(value_width)] + [rows_of(key_width)] * 2 + [line],
        out_specs=[
            rows_of(key_width),
            rows_of(key_width),
            pl.BlockSpec((key_width + 16, value_width), lambda n: (0, 0)),
        ],
        out_shape=[
            jax.ShapeDtypeStruct((tokens, key_width), bf16),
            jax.ShapeDtypeStruct((tokens, key_width), bf16),
            jax.ShapeDtypeStruct((key_width + 16, value_width), bf16),
        ],
        scratch_shapes=[
            pltpu.VMEM((key_width, value_width), f32),
            pltpu.VMEM((16, value_width), f32),
        ],
    )(query_rows, key_rows, value_rows, cosine, sine, running)
    return queries, keys, running, piece


def retention(
    queries, keys, running, pieces, value_rows, gate_rows, out_weight, rows_before
):
    tokens, key_width = queries.shape
    value_width = value_rows.shape[1]
    model_width = out_weight.shape[1]
    count = tokens // BLOCK
    members = lax.axis_size(TP)

    def rows_of(width):
        return pl.BlockSpec((BLOCK, width), lambda n, *_: (n, 0))

    line = pl.BlockSpec((1, 1, BLOCK), lambda n, *_: (n, 0, 0))
    where = jnp.reshape(lax.axis_index(EP), (1,)).astype(jnp.int32)
    return pl.pallas_call(
        mixer_kernel,
        grid_spec=pltpu.PrefetchScalarGridSpec(
            num_scalar_prefetch=1,
            grid=(count,),
            in_specs=[
                pl.BlockSpec(pieces.shape, lambda n, *_: (0, 0, 0)),
                rows_of(key_width),
                rows_of(key_width),
                rows_of(value_width),
                rows_of(value_width),
                line,
                pl.BlockSpec(out_weight.shape, lambda n, *_: (0, 0)),
            ],
            out_specs=pl.BlockSpec(
                (pl.Element(2), pl.Element(BLOCK // 2), pl.Element(model_width)),
                lambda n, *_: (2 * n, rows_before, 0),
            ),
            scratch_shapes=[pltpu.VMEM((key_width, value_width), f32)],
        ),
        out_shape=pltpu.HBM((members, rows_before + tokens // members, model_width), bf16),
        compiler_params=pltpu.CompilerParams(vmem_limit_bytes=40 * 2**20),
    )(where, pieces, queries, keys, value_rows, gate_rows, running, out_weight)


def local(
    query_rows,
    key_rows,
    value_rows,
    gate_rows,
    log_decay,
    out_weight,
    channel_input,
    norm_gain,
    routes,
    route_weight,
    expert_gate,
    expert_up,
    expert_down,
    shared_gate,
    shared_up,
    shared_down,
):
    tokens_here, topk = routes.shape
    model_width = channel_input.shape[1]
    experts_here = expert_gate.shape[0]
    ep_count, levels = lax.axis_size(EP), lax.axis_size("z")
    experts_all = ep_count * experts_here
    picks = tokens_here * topk
    capacity = picks // experts_all + max(2, picks // (3 * experts_all))
    experts = (expert_gate, expert_up, expert_down)

    widened = channel_input.astype(f32)
    normed = (
        widened * lax.rsqrt(jnp.mean(widened * widened, axis=-1, keepdims=True) + epsilon) * norm_gain
    ).astype(bf16)
    flat = routes.reshape(-1)
    order = jnp.arange(picks, dtype=jnp.int32)
    same = (flat[:, None] == flat[None, :]) & (order[None, :] < order[:, None])
    rank = jnp.sum(same.astype(jnp.int32), axis=1).reshape(tokens_here, topk)
    slots = routes * capacity + rank
    meta = jnp.concatenate([slots.astype(bf16), route_weight.astype(bf16)], axis=1)
    meta = jnp.pad(meta, ((0, 0), (0, LANES - 2 * topk)))

    padded = jnp.where(routes % experts_here == 0, routes // experts_here * SLOTS + rank, -1)
    spots = jnp.arange(ep_count * SLOTS, dtype=jnp.int32)
    fetch = [(spots[:, None] == padded[None, :, k]).astype(bf16) for k in range(topk)]
    sent = jnp.dot(sum(fetch), normed, preferred_element_type=f32).astype(bf16)
    sent = sent.reshape(ep_count, SLOTS, model_width)
    arrived = lax.all_to_all(sent, EP, split_axis=0, concat_axis=0, tiled=True)
    arrived = jnp.transpose(arrived[:, :capacity], (1, 0, 2)).reshape(1, -1, model_width)

    own = jnp.concatenate([normed, meta], axis=1)
    queries, keys, running, piece = own_state(query_rows, key_rows, value_rows, log_decay)
    piece = jnp.broadcast_to(piece, (ep_count,) + piece.shape)
    pieces = lax.all_to_all(piece, EP, split_axis=0, concat_axis=0, tiled=True)
    blocks = ring_gather(own, "z")
    arrived, blocks[levels // 2 - 1] = lax.optimization_barrier((arrived, blocks[levels // 2 - 1]))
    gathered = lax.all_gather(arrived, TP, axis=0, tiled=True)
    rows = jnp.concatenate(blocks, axis=0)
    rows, pieces = lax.optimization_barrier((rows, pieces))
    placed = [
        place(rows, e, experts_here, capacity, levels, ep_count) for e in range(1, experts_here)
    ]
    placed, pieces = lax.optimization_barrier((placed, pieces))
    exchanged = []
    for sent in placed:
        sent = sent.reshape(ep_count, levels * capacity, model_width)
        arrived = lax.all_to_all(sent, EP, split_axis=0, concat_axis=0, tiled=True)
        exchanged.append(arrived.reshape(-1, model_width))

    buffer = retention(
        queries, keys, running, pieces, value_rows, gate_rows, out_weight, gathered.shape[1]
    )
    buffer = grouped_mlp(gathered, *experts, 0, buffer)
    summed = lax.psum_scatter(buffer, TP, scatter_dimension=0, tiled=True)[0]
    mixer = summed[gathered.shape[1] :]
    exchanged, _ = lax.optimization_barrier((exchanged, buffer))

    results = []
    for e, arrived in enumerate(exchanged, 1):
        middle = arrived.shape[0] // 2
        halves = [swap(arrived[:middle]), swap(arrived[middle:])]
        halves = [swap(gated_mlp(half, *experts, e, parts=1)) for half in halves]
        both = gated_mlp(arrived, *experts, e, halves)
        both = both.reshape(ep_count, levels * capacity, model_width)
        back = lax.all_to_all(both, EP, split_axis=0, concat_axis=0, tiled=True)
        results.append(back.reshape(-1, model_width))

    shared = (shared_gate[None], shared_up[None], shared_down[None], 0)
    other = swap(gated_mlp(swap(rows), *shared))
    middle = rows.shape[0] // 2
    total = gated_mlp(rows, *shared, [other[:middle], other[middle:]])
    for e in range(1, experts_here):
        kind = bf16 if e == experts_here - 1 else f32
        total = collect(rows, results[e - 1], [total], e, experts_here, capacity, levels, kind)
    parts = [total[k * tokens_here : (k + 1) * tokens_here] for k in range(levels)]
    channel = ring_reduce(parts, "z")

    back = summed[: gathered.shape[1]].reshape(capacity, ep_count, model_width)
    back = jnp.pad(jnp.transpose(back, (1, 0, 2)), ((0, 0), (0, SLOTS - capacity), (0, 0)))
    returned = lax.all_to_all(back, EP, split_axis=0, concat_axis=0, tiled=True)
    returned = returned.reshape(-1, model_width)
    for k in range(topk):
        picked = jnp.dot(fetch[k].T, returned, preferred_element_type=f32)
        channel = channel + route_weight[:, k : k + 1] * picked
    return (mixer, channel.astype(bf16))


def solution(mesh):
    cores = 2
    split = Mesh(
        mesh.devices.reshape(4, 4, mesh.shape["tp"] // cores, cores), EP_TP
    )
    return jax.shard_map(
        local,
        mesh=split,
        in_specs=(
            P(EP, TP),
            P(EP, TP),
            P(EP, TP),
            P(EP, TP),
            P(TP, EP),
            P(TP, None),
            P(EP_TP, None),
            P(),
            P(EP_TP, None),
            P(EP_TP, None),
            P(EP, None, TP),
            P(EP, None, TP),
            P(EP, TP, None),
            P(None, TP),
            P(None, TP),
            P(TP, None),
        ),
        out_specs=(P(EP_TP, None), P(EP_TP, None)),
        check_vma=False,
    )
```
